512 devices in a mesh: dp: 4 (over x), kv: 64 (over z, y), tp: 2 (over core).
Axes of the slice: x: 4, y: 4, z: 16, core: 2. Of those that a mesh axis runs over, the one named last changes fastest.
Arguments:
- tokens: bfloat16 [256, 4096], P('dp', 'kv'), may hold values from -24 to 24
- positions: int32 [256], P(('dp', 'kv')), may hold values from 0 to 4095
- state: float32 [256, 16, 128, 128], P(('dp', 'kv'), 'tp'), may hold values from -0.6 to 0.6
- w_query: bfloat16 [4096, 2048], P('kv', 'tp'), may hold values from -0.09375 to 0.09375
- w_key: bfloat16 [4096, 2048], P('kv', 'tp'), may hold values from -0.09375 to 0.09375
- w_value: bfloat16 [4096, 2048], P('kv', 'tp'), may hold values from -0.09375 to 0.09375
- w_gate: bfloat16 [4096, 2048], P('kv', 'tp'), may hold values from -0.09375 to 0.09375
- w_out: bfloat16 [2048, 4096], P(None, ('kv', 'tp')), may hold values from -0.25 to 0.25
- gain_mix: float32 [4096], replicated, may hold values from 0.1 to 1.9
- w_ffn_gate: bfloat16 [4096, 11008], P(None, ('kv', 'tp')), may hold values from -0.09375 to 0.09375
- w_ffn_up: bfloat16 [4096, 11008], P(None, ('kv', 'tp')), may hold values from -0.09375 to 0.09375
- w_ffn_down: bfloat16 [11008, 4096], P(('kv', 'tp')), may hold values from -0.109375 to 0.109375
- gain_out: float32 [4096], replicated, may hold values from 0.1 to 1.9
Outputs:
- layer_out: bfloat16 [256, 4096], P('dp', ('kv', 'tp'))
- new_state: float32 [256, 16, 128, 128], P(('dp', 'kv'), 'tp')
The draws below stay inside these ranges and needn't reach their ends.
All inputs are finite; a program needn't handle non-finite values.
Results may differ from the reference program's by a relative error of at most 0.018.
Values may be sent and summed in bfloat16 or wider, within the bound.
No kernel may reach another device: no remote copies, remote signals or barrier semaphores. Data moves between devices by JAX's collectives and lax.ppermute only.
A program may use at most 64 MiB of HBM per device.

```python
import jax
import jax.numpy as jnp
from jax import lax

D = 4096
HEADS = 16
HEAD_DIM = 128
FF = 11008
BATCH = 256


def draw_tokens(key, part):
    normal_key = jax.random.fold_in(jax.random.fold_in(key, 11), 0)
    columns = jnp.arange(D, dtype=jnp.float32) / D
    column_scale = 0.5 * 4.0 ** columns
    base = jnp.clip(jax.random.normal(normal_key, (BATCH, D), jnp.float32), -6.0, 6.0)
    values = base * column_scale[None, :]
    return jnp.clip(values, -24.0, 24.0).astype(jnp.bfloat16)


def with_ends(entries, rng, least, top_value):
    shape = entries.shape
    place = [jax.random.randint(jax.random.fold_in(rng, axis), (), 0, shape[axis]) for axis in range(len(shape))]
    entries = entries.at[tuple(place)].set(least)
    longest = shape.index(max(shape))
    place[longest] = (place[longest] + 1) % shape[longest]
    return entries.at[tuple(place)].set(top_value)


def block_levels(own_key, dims, cuts, low, largest):
    def one(position, shards_of):
        steps = jax.random.uniform(jax.random.fold_in(jax.random.fold_in(own_key, 6), position), (shards_of,), jnp.float32, low / len(cuts), largest / len(cuts))
        return jnp.repeat(jnp.exp(steps), dims[position] // shards_of).reshape((-1,) + (1,) * (len(dims) - position - 1))

    level = one(*cuts[0])
    for cut in cuts[1:]:
        level = level * one(*cut)
    return level


def normal_values(rng, shape, scale, bound, cuts=(), held_as=jnp.bfloat16):
    values = jax.random.normal(rng, shape, jnp.float32) * scale
    if len(cuts) > 0:
        values = block_levels(rng, shape, cuts, -0.22, 0.18) * values
    return jnp.clip(values, min=-bound, max=bound).astype(held_as)


def setup_inputs(seed: int = 0) -> dict:
    seeds = jax.random.split(jax.random.key(seed), 14)
    return {
        "tokens": draw_tokens(jax.random.fold_in(seeds[13], 71), 0),
        "positions": with_ends(jax.random.randint(seeds[1], (BATCH,), 0, 4096), jax.random.fold_in(seeds[1], 1), 0, 4095).astype(jnp.int32),
        "state": normal_values(seeds[2], (BATCH, HEADS, HEAD_DIM, HEAD_DIM), 0.1, 0.6, ((0, 256), (1, 2)), jnp.float32),
        "w_query": normal_values(seeds[3], (D, HEADS * HEAD_DIM), D ** -0.5, 0.09375, ((0, 64), (1, 2))),
        "w_key": normal_values(seeds[4], (D, HEADS * HEAD_DIM), D ** -0.5, 0.09375, ((0, 64), (1, 2))),
        "w_value": normal_values(seeds[5], (D, HEADS * HEAD_DIM), D ** -0.5, 0.09375, ((0, 64), (1, 2))),
        "w_gate": normal_values(seeds[6], (D, HEADS * HEAD_DIM), D ** -0.5, 0.09375, ((0, 64), (1, 2))),
        "w_out": normal_values(seeds[7], (HEADS * HEAD_DIM, D), (HEADS * HEAD_DIM // 4) ** -0.5, 0.25, ((1, 128),)),
        "gain_mix": jnp.clip(1.0 + 0.18 * jax.random.normal(seeds[8], (D,), jnp.float32), 0.1, 1.9),
        "w_ffn_gate": normal_values(seeds[9], (D, FF), D ** -0.5, 0.09375, ((1, 128),)),
        "w_ffn_up": normal_values(seeds[10], (D, FF), D ** -0.5, 0.09375, ((1, 128),)),
        "w_ffn_down": normal_values(seeds[11], (FF, D), (FF // 4) ** -0.5, 0.109375, ((0, 128),)),
        "gain_out": jnp.clip(1.0 + 0.18 * jax.random.normal(seeds[12], (D,), jnp.float32), 0.1, 1.9),
    }


def rotate(vectors, positions):
    half = vectors.shape[-1] // 2
    inverse = 10000.0 ** (-jnp.arange(half, dtype=jnp.float32) / half)
    angle = positions.astype(jnp.float32)[:, None, None] * inverse[None, None, :]
    cosine = jnp.cos(angle)
    sine = jnp.sin(angle)
    first = vectors[..., :half]
    second = vectors[..., half:]
    return jnp.concatenate([first * cosine - second * sine, first * sine + second * cosine], -1)

def layer_norm(values, gain):
    count = values.shape[-1]
    mean = lax.optimization_barrier(jnp.sum(values, -1, keepdims=True)) / count
    var = lax.optimization_barrier(jnp.sum(values * values, -1, keepdims=True)) / count - mean * mean
    return (values - mean) * lax.rsqrt(var + 1e-05) * gain

def reference(tokens, positions, state, w_query, w_key, w_value, w_gate, w_out, gain_mix, w_ffn_gate, w_ffn_up, w_ffn_down, gain_out):
    rows = tokens.shape[0]
    heads = state.shape[1]
    width_head = state.shape[2]
    query = jnp.dot(tokens, w_query, preferred_element_type=jnp.float32).reshape(rows, heads, width_head)
    key = jnp.dot(tokens, w_key, preferred_element_type=jnp.float32).reshape(rows, heads, width_head)
    value = jnp.dot(tokens, w_value, preferred_element_type=jnp.float32).reshape(rows, heads, width_head)
    gate_pre = jnp.dot(tokens, w_gate, preferred_element_type=jnp.float32)
    query = rotate(query, positions)
    key = rotate(key, positions) * width_head ** (-0.5)
    head_ids = jnp.arange(heads, dtype=jnp.float32)
    decay = 1.0 - 2.0 ** (-5.0 - 6.0 * head_ids / (heads - 1))
    new_state = decay[None, :, None, None] * state + key[:, :, :, None] * value[:, :, None, :]
    retained = jnp.einsum('bhd,bhdv->bhv', query, new_state, precision=lax.Precision.HIGHEST)
    mean = lax.optimization_barrier(jnp.mean(retained, -1, keepdims=True))
    var = lax.optimization_barrier(jnp.mean(jnp.square(retained - mean), -1, keepdims=True))
    normed = (retained - mean) * lax.rsqrt(var + 1e-05)
    attended = (normed.reshape(rows, heads * width_head) * jax.nn.silu(gate_pre)).astype(jnp.bfloat16)
    mixed = jnp.dot(attended, w_out, preferred_element_type=jnp.float32)
    mixed_pre = (tokens.astype(jnp.float32) + mixed).astype(jnp.bfloat16)
    hidden = layer_norm(mixed_pre.astype(jnp.float32), gain_mix).astype(jnp.bfloat16)
    gate = jnp.dot(hidden, w_ffn_gate, preferred_element_type=jnp.float32)
    upward = jnp.dot(hidden, w_ffn_up, preferred_element_type=jnp.float32)
    inner = (jax.nn.silu(gate) * upward).astype(jnp.bfloat16)
    ffn = jnp.dot(inner, w_ffn_down, preferred_element_type=jnp.float32)
    layer_out = layer_norm(hidden.astype(jnp.float32) + ffn, gain_out).astype(jnp.bfloat16)
    return (layer_out, new_state)
```

```python
import jax
import jax.numpy as jnp
from jax import lax
from jax.experimental import pallas as pl
from jax.experimental.pallas import tpu as pltpu
from jax.sharding import Mesh
from jax.sharding import PartitionSpec as P

KV = ("kv_0", "kv_1")
YZ = ("kv_1", "kv_0")
Y_TP = ("kv_1", "tp")
KV_TP = ("kv_0", "kv_1", "tp")
DP_KV = ("dp", "kv_0", "kv_1")
F32 = jnp.float32
BF16 = jnp.bfloat16
LANES = 128
NZ = 16
NY = 4
SEQS = NZ * NY
INTERPRET = False

VMEM = pl.BlockSpec(memory_space=pltpu.VMEM)
SMEM = pl.BlockSpec(memory_space=pltpu.SMEM)


def kernel_call(body, out_shape, n_in, scalars=0, scratch=(), name=None):
    single = not isinstance(out_shape, (list, tuple))
    return pl.pallas_call(
        body,
        out_shape=out_shape,
        in_specs=[SMEM] * scalars + [VMEM] * (n_in - scalars),
        out_specs=VMEM if single else [VMEM] * len(out_shape),
        scratch_shapes=list(scratch),
        compiler_params=pltpu.CompilerParams(vmem_limit_bytes=40 * 1024 * 1024),
        interpret=INTERPRET,
        name=name,
    )


def sds(shape, dtype):
    return jax.ShapeDtypeStruct(shape, dtype)


def rows_of(s):
    return (s % NY) * NZ + s // NY


def perm_matrix(dtype):
    d = lax.broadcasted_iota(jnp.int32, (SEQS, SEQS), 0)
    s = lax.broadcasted_iota(jnp.int32, (SEQS, SEQS), 1)
    return (d == rows_of(s)).astype(F32).astype(dtype)


def mm(a, b, ca, cb):
    return lax.dot_general(a, b, (((ca,), (cb,)), ((), ())), preferred_element_type=F32)


def project_kernel(tok_hbm, wq, wk, wv, wg, out, tok, weights, sems):
    sources = (wq, wk, wv, wg)
    copies = [pltpu.make_async_copy(tok_hbm, tok, sems.at[4])]
    for i, w in enumerate(sources):
        copies.append(pltpu.make_async_copy(w, weights.at[i], sems.at[i]))
    for copy in copies:
        copy.start()
    copies[0].wait()
    rows = mm(perm_matrix(BF16), tok[...], 1, 0).astype(BF16)
    width = weights.shape[2]
    for i in range(len(sources)):
        copies[1 + i].wait()
        part = mm(rows, weights[i], 1, 0).astype(BF16)
        for y in range(NY):
            out[y, :, i * width : (i + 1) * width] = part[y * NZ : (y + 1) * NZ]


def near_sum_kernel(x, out, wide):
    for c in range(wide.shape[1]):
        cols = slice(c * LANES, (c + 1) * LANES)
        total = x[0, :, cols].astype(F32)
        for y in range(1, NY):
            total += x[y, :, cols].astype(F32)
        wide[:, c, :] = total
    out[...] = wide[...].astype(BF16)


def retention_kernel(x, aux, state, new_state, out):
    heads, dim = state.shape[1], state.shape[2]
    total = x[0].astype(F32)
    for z in range(1, NZ):
        total += x[z].astype(F32)
    cosine = aux[0:1, :]
    sine = aux[1:2, :]
    query = total[0:heads]
    key = total[heads : 2 * heads]
    value = total[2 * heads : 3 * heads]
    gate = total[3 * heads : 4 * heads]
    query = query * cosine + pltpu.roll(query, dim // 2, 1) * sine
    key = (key * cosine + pltpu.roll(key, dim // 2, 1) * sine) * dim ** (-0.5)
    query_t = query.T
    key_t = key.T
    lines = []
    for h in range(heads):
        updated = aux[8 + h : 9 + h, :] * state[0, h] + key_t[:, h : h + 1] * value[h : h + 1, :]
        new_state[0, h] = updated
        lines.append(jnp.sum(query_t[:, h : h + 1] * updated, axis=0, keepdims=True))
    retained = jnp.concatenate(lines, axis=0)
    mean = jnp.mean(retained, -1, keepdims=True)
    var = jnp.mean(jnp.square(retained - mean), -1, keepdims=True)
    normed = (retained - mean) * lax.rsqrt(var + 1e-05)
    silu = gate / (1.0 + jnp.exp(-gate))
    attended = (normed * silu).astype(BF16)
    out[...] = jnp.broadcast_to(attended[None], out.shape)


def mix_kernel(where, x, w_t, tok, out, wide):
    tp = where[0]
    tps, seqs, heads, dim = x.shape
    cols = w_t.shape[0]
    groups = LANES // cols
    wide[...] = x[...].astype(F32)
    own = lax.broadcasted_iota(jnp.int32, (tok.shape[1], LANES), 0)
    lane = lax.broadcasted_iota(jnp.int32, (tok.shape[1], LANES), 1)
    pick = (own == tp * cols + lane % cols).astype(F32).astype(BF16)
    rows = mm(perm_matrix(BF16), tok[...], 1, 0).astype(BF16)
    acc = mm(rows, pick, 1, 0)
    w4 = jnp.concatenate([w_t[...]] * groups, axis=0)
    for t in range(tps):
        for h in range(heads):
            k = (t * heads + h) * dim
            acc += mm(wide[t, :, h, :].astype(BF16), w4[:, k : k + dim], 1, 1)
    block = lax.broadcasted_iota(jnp.int32, (seqs // groups, LANES), 1) // cols
    per = seqs // groups
    packed = acc[0:per]
    for g in range(1, groups):
        packed = jnp.where(block == g, acc[g * per : (g + 1) * per], packed)
    out[...] = jnp.broadcast_to(packed.astype(BF16)[None], out.shape)


def feed_kernel(where, x, gain, wg_t, wu_t, wd, out, row, wide, narrow, sums_out):
    per = x.shape[2]
    tps = x.shape[0] // NY
    groups = SEQS // per
    cols = LANES // groups
    chips = LANES // (tps * cols)
    width = wide.shape[1]
    lane = lax.broadcasted_iota(jnp.int32, (per, LANES), 1) // cols
    sums = [jnp.zeros((per, LANES), F32) for _ in range(groups)]
    squares = [jnp.zeros((per, LANES), F32) for _ in range(groups)]
    for a in range(SEQS // chips):
        tiles = [None] * groups
        for q in range(groups):
            kv = a * chips + q // tps
            source = x[(kv % NY) * tps + q % tps, kv // NY].astype(F32)
            for g in range(groups):
                shift = ((q - g) * cols) % LANES
                moved = source if shift == 0 else pltpu.roll(source, shift, 1)
                tiles[g] = moved if q == 0 else jnp.where(lane == q, moved, tiles[g])
        for g in range(groups):
            wide[g * per : (g + 1) * per, a * LANES : (a + 1) * LANES] = tiles[g]
            sums[g] += tiles[g]
            squares[g] += tiles[g] * tiles[g]
    mean = jnp.sum(jnp.concatenate(sums, 0), -1, keepdims=True) / width
    var = jnp.sum(jnp.concatenate(squares, 0), -1, keepdims=True) / width - mean * mean
    scale = lax.rsqrt(var + 1e-05)
    for a in range(width // LANES):
        c = slice(a * LANES, (a + 1) * LANES)
        hidden = ((wide[:, c] - mean) * scale * gain[:, c]).astype(BF16)
        narrow[:, c] = hidden
        wide[:, c] = hidden.astype(F32)
    row[...] = wide[pl.ds(where[1], 1), :]
    gate = mm(narrow[...], wg_t[...], 1, 1)
    up = mm(narrow[...], wu_t[...], 1, 1)
    inner = (gate / (1.0 + jnp.exp(-gate)) * up).astype(BF16)
    lines = sums_out.shape[1]
    for c in range(lines):
        sums_out[:, c, :] = mm(inner, wd[:, c * LANES : (c + 1) * LANES], 1, 0)
    half = lines // tps
    for y in range(NY):
        for t in range(tps):
            block = sums_out[y * NZ : (y + 1) * NZ, t * half : (t + 1) * half, :]
            out[y * tps + t] = block.astype(BF16)


def plain_sum_kernel(x, out):
    total = x[0].astype(F32)
    for d in range(1, x.shape[0]):
        total += x[d].astype(F32)
    out[...] = total.astype(BF16)


def ffn_sum_kernel(where, x, hidden, out):
    per = x.shape[1]
    total = hidden[pl.ds(pl.multiple_of(where[0] * per, per), per), :]
    for d in range(x.shape[0]):
        total += x[d].astype(F32)
    out[...] = total


def total_of(x):
    return jnp.sum(jnp.sum(x, 0, keepdims=True), 1, keepdims=True)


def final_norm_kernel(x, gain, out):
    p = x[...]
    count = p.shape[0] * p.shape[1]
    mean = total_of(p) / count
    var = total_of(p * p) / count - mean * mean
    normed = ((p - mean) * lax.rsqrt(var + 1e-05) * gain[...]).astype(BF16)
    lines = p.shape[0]
    d = lax.broadcasted_iota(jnp.int32, (SEQS, lines), 0)
    line = lax.broadcasted_iota(jnp.int32, (SEQS, lines), 1)
    kv = (d % NZ) * NY + d // NZ
    spread = (kv * lines // SEQS == line).astype(F32).astype(BF16)
    out[...] = mm(spread, normed, 1, 0)


def place_kernel(where, x, out, wide):
    wide[...] = mm(x[...].astype(BF16), perm_matrix(BF16), 0, 0)
    cols = out.shape[0]
    out[...] = wide[pl.ds(pl.multiple_of(where[2], cols), cols), :].astype(BF16)


def on_device(
    tokens,
    positions,
    state,
    w_query,
    w_key,
    w_value,
    w_gate,
    w_out,
    gain_mix,
    w_ffn_gate,
    w_ffn_up,
    w_ffn_down,
    gain_out,
):
    heads, dim = state.shape[1], state.shape[2]
    width = w_ffn_gate.shape[0]
    cols = w_out.shape[1]
    proj = 4 * heads
    half = width // 2
    tp = lax.axis_index("tp")
    place = lax.axis_index("kv_1") * NZ + lax.axis_index("kv_0")
    offset = (lax.axis_index("kv_1") % 2) * (2 * cols) + tp * cols
    where = jnp.stack([tp, place, offset]).astype(jnp.int32)

    inverse = 10000.0 ** (-jnp.arange(dim // 2, dtype=F32) / (dim // 2))
    angle = positions.astype(F32)[:, None] * inverse[None, :]
    cosine = jnp.cos(angle)
    sine = jnp.sin(angle)
    head_ids = (tp * heads + jnp.arange(heads, dtype=jnp.int32)).astype(F32)
    decay = 1.0 - 2.0 ** (-5.0 - 6.0 * head_ids / (2 * heads - 1))
    aux = jnp.concatenate(
        [
            jnp.concatenate([cosine, cosine], 1),
            jnp.concatenate([-sine, sine], 1),
            jnp.zeros((6, dim), F32),
            jnp.broadcast_to(decay[:, None], (heads, dim)),
        ],
        0,
    )

    tokens_in, aux, where = lax.optimization_barrier((tokens, aux, where))
    parts = pl.pallas_call(
        project_kernel,
        out_shape=sds((NY, NZ, proj * dim), BF16),
        in_specs=[pl.BlockSpec(memory_space=pl.ANY)] * 5,
        out_specs=VMEM,
        scratch_shapes=[
            pltpu.VMEM(tokens.shape, BF16),
            pltpu.VMEM((4, *w_query.shape), BF16),
            pltpu.SemaphoreType.DMA((5,)),
        ],
        interpret=INTERPRET,
        name="project",
    )(tokens_in, w_query, w_key, w_value, w_gate)
    near = lax.all_to_all(parts, "kv_1", 0, 0, tiled=True)
    near = kernel_call(
        near_sum_kernel,
        sds((NZ, proj, dim), BF16),
        1,
        scratch=[pltpu.VMEM((NZ, proj, dim), F32)],
        name="near_sum",
    )(near)
    far = lax.all_to_all(near, "kv_0", 0, 0, tiled=True)
    new_state, attended = kernel_call(
        retention_kernel,
        [sds(state.shape, F32), sds((SEQS, heads, dim), BF16)],
        3,
        name="retention",
    )(far, aux, state)
    gathered = lax.all_to_all(attended, YZ, 0, 0, tiled=True)
    gathered = lax.all_gather(gathered, "tp", axis=0)
    per = SEQS * cols // LANES
    mixed = kernel_call(
        mix_kernel,
        sds((NZ, per, LANES), BF16),
        4,
        scalars=1,
        scratch=[pltpu.VMEM((2, SEQS, heads, dim), F32)],
        name="mix",
    )(where, gathered.reshape(2, SEQS, heads, dim), w_out.T, tokens)
    rows = lax.all_to_all(mixed, "kv_0", 0, 0, tiled=True)
    rows = jnp.broadcast_to(rows[None], (2 * NY, *rows.shape))
    rows = lax.all_to_all(rows, Y_TP, 0, 0, tiled=True)
    lines = half // LANES
    part, hidden_row = kernel_call(
        feed_kernel,
        [sds((2 * NY, NZ, lines, LANES), BF16), sds((1, width), F32)],
        6,
        scalars=1,
        scratch=[
            pltpu.VMEM((SEQS, width), F32),
            pltpu.VMEM((SEQS, width), BF16),
            pltpu.VMEM((SEQS, 2 * lines, LANES), F32),
        ],
        name="feed",
    )(where, rows, gain_mix[None, :], w_ffn_gate.T, w_ffn_up.T, w_ffn_down)
    part = lax.all_to_all(part, Y_TP, 0, 0, tiled=True)
    part = kernel_call(plain_sum_kernel, sds((NZ, lines, LANES), BF16), 1, name="half_sum")(part)
    part = lax.all_to_all(part, "kv_0", 0, 0, tiled=True)
    summed = kernel_call(
        ffn_sum_kernel, sds((lines, LANES), F32), 3, scalars=1, name="ffn_sum"
    )(where, part, hidden_row.reshape(2 * lines, LANES))
    summed = lax.all_gather(summed, "tp", axis=0, tiled=True)
    spread = kernel_call(final_norm_kernel, sds((SEQS, LANES), F32), 2, name="final_norm")(
        summed, gain_out.reshape(2 * lines, LANES)
    )
    spread = lax.all_to_all(spread.reshape(SEQS, 1, LANES), YZ, 0, 0, tiled=True)
    layer_out = kernel_call(
        place_kernel,
        sds((cols, SEQS), BF16),
        2,
        scalars=1,
        scratch=[pltpu.VMEM((LANES, SEQS), F32)],
        name="place",
    )(where, spread.reshape(SEQS, LANES))
    return (layer_out.T, new_state)


def solution(mesh):
    finer = Mesh(
        mesh.devices.reshape(mesh.shape["dp"], NZ, NY, mesh.shape["tp"]),
        ("dp", "kv_0", "kv_1", "tp"),
    )
    return jax.shard_map(
        on_device,
        mesh=finer,
        in_specs=(
            P("dp", KV),
            P(DP_KV),
            P(DP_KV, "tp", None, None),
            P(KV, "tp"),
            P(KV, "tp"),
            P(KV, "tp"),
            P(KV, "tp"),
            P(None, KV_TP),
            P(),
            P(None, KV_TP),
            P(None, KV_TP),
            P(KV_TP, None),
            P(),
        ),
        out_specs=(P("dp", KV_TP), P(DP_KV, "tp", None, None)),
        check_vma=False,
    )
```

```python
import jax
import jax.numpy as jnp
from jax import lax
from jax.experimental import pallas as pl
from jax.experimental.pallas import tpu as pltpu
from jax.sharding import Mesh
from jax.sharding import PartitionSpec as P

KV = ("kv_0", "kv_1")
YZ = ("kv_1", "kv_0")
KV_TP = ("kv_0", "kv_1", "tp")
DP_KV = ("dp", "kv_0", "kv_1")
F32 = jnp.float32
BF16 = jnp.bfloat16
LANES = 128
NZ = 16
NY = 4
SEQS = NZ * NY
INTERPRET = False

VMEM = pl.BlockSpec(memory_space=pltpu.VMEM)
PARAMS = pltpu.CompilerParams(vmem_limit_bytes=32 * 1024 * 1024)


def kernel_call(body, out_shape, n_in, scratch=(), name=None):
    single = not isinstance(out_shape, (list, tuple))
    return pl.pallas_call(
        body,
        out_shape=out_shape,
        in_specs=[VMEM] * n_in,
        out_specs=VMEM if single else [VMEM] * len(out_shape),
        scratch_shapes=list(scratch),
        compiler_params=PARAMS,
        interpret=INTERPRET,
        name=name,
    )


def sds(shape, dtype):
    return jax.ShapeDtypeStruct(shape, dtype)


def rows_of(s):
    return (s % NY) * NZ + s // NY


def perm_matrix(dtype):
    d = lax.broadcasted_iota(jnp.int32, (SEQS, SEQS), 0)
    s = lax.broadcasted_iota(jnp.int32, (SEQS, SEQS), 1)
    return (d == rows_of(s)).astype(F32).astype(dtype)


def mm(a, b, ca, cb):
    return lax.dot_general(a, b, (((ca,), (cb,)), ((), ())), preferred_element_type=F32)


def project_kernel(tok_hbm, wq, wk, wv, wg, out, tok, weights, sems):
    sources = (wq, wk, wv, wg)
    copies = [pltpu.make_async_copy(tok_hbm, tok, sems.at[4])]
    for i, w in enumerate(sources):
        copies.append(pltpu.make_async_copy(w, weights.at[i], sems.at[i]))
    for copy in copies:
        copy.start()
    copies[0].wait()
    rows = mm(perm_matrix(BF16), tok[...], 1, 0).astype(BF16)
    width = weights.shape[2]
    for i in range(len(sources)):
        copies[1 + i].wait()
        part = mm(rows, weights[i], 1, 0).astype(BF16)
        for y in range(NY):
            out[y, :, i * width : (i + 1) * width] = part[y * NZ : (y + 1) * NZ]


def near_sum_kernel(x, out, wide):
    for c in range(wide.shape[1]):
        cols = slice(c * LANES, (c + 1) * LANES)
        total = x[0, :, cols].astype(F32)
        for y in range(1, NY):
            total += x[y, :, cols].astype(F32)
        wide[:, c, :] = total
    out[...] = wide[...].astype(BF16)


def retention_kernel(x, aux, state, new_state, out):
    heads, dim = state.shape[1], state.shape[2]
    total = x[0].astype(F32)
    for z in range(1, NZ):
        total += x[z].astype(F32)
    cosine = aux[0:1, :]
    sine = aux[1:2, :]
    query = total[0:heads]
    key = total[heads : 2 * heads]
    value = total[2 * heads : 3 * heads]
    gate = total[3 * heads : 4 * heads]
    query = query * cosine + pltpu.roll(query, dim // 2, 1) * sine
    key = (key * cosine + pltpu.roll(key, dim // 2, 1) * sine) * dim ** (-0.5)
    query_t = query.T
    key_t = key.T
    lines = []
    for h in range(heads):
        updated = aux[8 + h : 9 + h, :] * state[0, h] + key_t[:, h : h + 1] * value[h : h + 1, :]
        new_state[0, h] = updated
        lines.append(jnp.sum(query_t[:, h : h + 1] * updated, axis=0, keepdims=True))
    retained = jnp.concatenate(lines, axis=0)
    mean = jnp.mean(retained, -1, keepdims=True)
    var = jnp.mean(jnp.square(retained - mean), -1, keepdims=True)
    normed = (retained - mean) * lax.rsqrt(var + 1e-05)
    silu = gate / (1.0 + jnp.exp(-gate))
    attended = (normed * silu).astype(BF16)
    out[...] = jnp.broadcast_to(attended[None], out.shape)


def mix_kernel(x, w_t, tok, out, wide):
    tp = lax.axis_index("tp")
    tps, seqs, heads, dim = x.shape
    cols = w_t.shape[0]
    groups = LANES // cols
    wide[...] = x[...].astype(F32)
    own = lax.broadcasted_iota(jnp.int32, (tok.shape[1], LANES), 0)
    lane = lax.broadcasted_iota(jnp.int32, (tok.shape[1], LANES), 1)
    pick = (own == tp * cols + lane % cols).astype(F32).astype(BF16)
    rows = mm(perm_matrix(BF16), tok[...], 1, 0).astype(BF16)
    acc = mm(rows, pick, 1, 0)
    w4 = jnp.concatenate([w_t[...]] * groups, axis=0)
    for t in range(tps):
        for h in range(heads):
            k = (t * heads + h) * dim
            acc += mm(wide[t, :, h, :].astype(BF16), w4[:, k : k + dim], 1, 1)
    block = lax.broadcasted_iota(jnp.int32, (seqs // groups, LANES), 1) // cols
    per = seqs // groups
    packed = acc[0:per]
    for g in range(1, groups):
        packed = jnp.where(block == g, acc[g * per : (g + 1) * per], packed)
    out[...] = jnp.broadcast_to(packed.astype(BF16)[None], out.shape)


def feed_kernel(x, gain, wg_t, wu_t, wd, own, other, row, wide, narrow, sums_out):
    tps = x.shape[0]
    per = x.shape[3]
    tp = lax.axis_index("tp")
    place = lax.axis_index("kv_1") * NZ + lax.axis_index("kv_0")
    groups = SEQS // per
    cols = LANES // groups
    chips = LANES // (tps * cols)
    width = wide.shape[1]
    lane = lax.broadcasted_iota(jnp.int32, (per, LANES), 1) // cols
    sums = [jnp.zeros((per, LANES), F32) for _ in range(groups)]
    squares = [jnp.zeros((per, LANES), F32) for _ in range(groups)]
    for a in range(SEQS // chips):
        tiles = [None] * groups
        for q in range(groups):
            kv = a * chips + q // tps
            source = x[q % tps, kv % NY, kv // NY].astype(F32)
            for g in range(groups):
                shift = ((q - g) * cols) % LANES
                moved = source if shift == 0 else pltpu.roll(source, shift, 1)
                tiles[g] = moved if q == 0 else jnp.where(lane == q, moved, tiles[g])
        for g in range(groups):
            wide[g * per : (g + 1) * per, a * LANES : (a + 1) * LANES] = tiles[g]
            sums[g] += tiles[g]
            squares[g] += tiles[g] * tiles[g]
    mean = jnp.sum(jnp.concatenate(sums, 0), -1, keepdims=True) / width
    var = jnp.sum(jnp.concatenate(squares, 0), -1, keepdims=True) / width - mean * mean
    scale = lax.rsqrt(var + 1e-05)
    for a in range(width // LANES):
        c = slice(a * LANES, (a + 1) * LANES)
        hidden = ((wide[:, c] - mean) * scale * gain[:, c]).astype(BF16)
        narrow[:, c] = hidden
        wide[:, c] = hidden.astype(F32)
    row[...] = wide[pl.ds(place, 1), :]
    gate = mm(narrow[...], wg_t[...], 1, 1)
    up = mm(narrow[...], wu_t[...], 1, 1)
    inner = (gate / (1.0 + jnp.exp(-gate)) * up).astype(BF16)
    half = own.shape[1]
    step = 4
    for t in range(tps):
        for c in range(0, half, step):
            k = (t * half + c) * LANES
            part = mm(inner, wd[:, k : k + step * LANES], 1, 0)
            for i in range(step):
                sums_out[t, :, c + i, :] = part[:, i * LANES : (i + 1) * LANES]
    own[...] = sums_out[tp].astype(BF16)
    other[...] = sums_out[1 - tp].astype(BF16)


def pair_sum_kernel(own, both, out):
    tp = lax.axis_index("tp")
    out[...] = (own[...].astype(F32) + both[1 - tp].astype(F32)).astype(BF16)


def plain_sum_kernel(x, out):
    total = x[0].astype(F32)
    for d in range(1, x.shape[0]):
        total += x[d].astype(F32)
    out[...] = total.astype(BF16)


def ffn_sum_kernel(x, hidden, out):
    per = x.shape[1]
    tp = lax.axis_index("tp")
    total = hidden[pl.ds(pl.multiple_of(tp * per, per), per), :]
    for d in range(x.shape[0]):
        total += x[d].astype(F32)
    out[...] = total


def total_of(x):
    return jnp.sum(jnp.sum(x, 0, keepdims=True), 1, keepdims=True)


def final_norm_kernel(x, gain, out):
    p = x[...]
    count = p.shape[0] * p.shape[1]
    mean = total_of(p) / count
    var = total_of(p * p) / count - mean * mean
    normed = ((p - mean) * lax.rsqrt(var + 1e-05) * gain[...]).astype(BF16)
    lines = p.shape[0]
    d = lax.broadcasted_iota(jnp.int32, (SEQS, lines), 0)
    line = lax.broadcasted_iota(jnp.int32, (SEQS, lines), 1)
    spread = (d * lines // SEQS == line).astype(F32).astype(BF16)
    out[...] = mm(spread, normed, 1, 0)


def place_kernel(x, out):
    cols = out.shape[0]
    offset = (lax.axis_index("kv_1") % 2) * (2 * cols) + lax.axis_index("tp") * cols
    col = lax.broadcasted_iota(jnp.int32, (cols, LANES), 0)
    lane = lax.broadcasted_iota(jnp.int32, (cols, LANES), 1)
    pick = (lane == col + offset).astype(F32).astype(BF16)
    out[...] = mm(pick, x[...].astype(BF16), 1, 1).astype(BF16)


def on_device(
    tokens,
    positions,
    state,
    w_query,
    w_key,
    w_value,
    w_gate,
    w_out,
    gain_mix,
    w_ffn_gate,
    w_ffn_up,
    w_ffn_down,
    gain_out,
):
    heads, dim = state.shape[1], state.shape[2]
    width = w_ffn_gate.shape[0]
    cols = w_out.shape[1]
    proj = 4 * heads
    half = width // 2
    tp = lax.axis_index("tp")

    inverse = 10000.0 ** (-jnp.arange(dim // 2, dtype=F32) / (dim // 2))
    angle = positions.astype(F32)[:, None] * inverse[None, :]
    cosine = jnp.cos(angle)
    sine = jnp.sin(angle)
    head_ids = (tp * heads + jnp.arange(heads, dtype=jnp.int32)).astype(F32)
    decay = 1.0 - 2.0 ** (-5.0 - 6.0 * head_ids / (2 * heads - 1))
    aux = jnp.concatenate(
        [
            jnp.concatenate([cosine, cosine], 1),
            jnp.concatenate([-sine, sine], 1),
            jnp.zeros((6, dim), F32),
            jnp.broadcast_to(decay[:, None], (heads, dim)),
        ],
        0,
    )

    tokens_in, aux = lax.optimization_barrier((tokens, aux))
    parts = pl.pallas_call(
        project_kernel,
        out_shape=sds((NY, NZ, proj * dim), BF16),
        in_specs=[pl.BlockSpec(memory_space=pltpu.HBM)] * 5,
        out_specs=VMEM,
        scratch_shapes=[
            pltpu.VMEM(tokens.shape, BF16),
            pltpu.VMEM((4, *w_query.shape), BF16),
            pltpu.SemaphoreType.DMA((5,)),
        ],
        compiler_params=PARAMS,
        interpret=INTERPRET,
        name="project",
    )(tokens_in, w_query, w_key, w_value, w_gate)
    near = lax.all_to_all(parts, "kv_1", 0, 0, tiled=True)
    near = kernel_call(
        near_sum_kernel,
        sds((NZ, proj, dim), BF16),
        1,
        scratch=[pltpu.VMEM((NZ, proj, dim), F32)],
        name="near_sum",
    )(near)
    far = lax.all_to_all(near, "kv_0", 0, 0, tiled=True)
    new_state, attended = kernel_call(
        retention_kernel,
        [sds(state.shape, F32), sds((SEQS, heads, dim), BF16)],
        3,
        name="retention",
    )(far, aux, state)
    gathered = lax.all_to_all(attended, YZ, 0, 0, tiled=True)
    gathered = lax.all_gather(gathered, "tp", axis=0)
    per = SEQS * cols // LANES
    mixed = kernel_call(
        mix_kernel,
        sds((NZ, per, LANES), BF16),
        3,
        scratch=[pltpu.VMEM((2, SEQS, heads, dim), F32)],
        name="mix",
    )(gathered.reshape(2, SEQS, heads, dim), w_out.T, tokens)
    rows = lax.all_to_all(mixed, "kv_0", 0, 0, tiled=True)
    rows = jnp.broadcast_to(rows[None], (NY, *rows.shape))
    rows = lax.all_to_all(rows, "kv_1", 0, 0, tiled=True)
    rows = lax.all_gather(rows, "tp", axis=0)
    lines = half // LANES
    own, other, hidden_row = kernel_call(
        feed_kernel,
        [sds((SEQS, lines, LANES), BF16)] * 2 + [sds((1, width), F32)],
        5,
        scratch=[
            pltpu.VMEM((SEQS, width), F32),
            pltpu.VMEM((SEQS, width), BF16),
            pltpu.VMEM((2, SEQS, lines, LANES), F32),
        ],
        name="feed",
    )(rows, gain_mix[None, :], w_ffn_gate.T, w_ffn_up.T, w_ffn_down)
    both = lax.all_gather(other, "tp", axis=0)
    part = kernel_call(pair_sum_kernel, sds(own.shape, BF16), 2, name="pair_sum")(own, both)
    part = part.reshape(NY, NZ, lines, LANES)
    part = lax.all_to_all(part, "kv_1", 0, 0, tiled=True)
    part = kernel_call(plain_sum_kernel, sds((NZ, lines, LANES), BF16), 1, name="half_sum")(part)
    part = lax.all_to_all(part, "kv_0", 0, 0, tiled=True)
    summed = kernel_call(ffn_sum_kernel, sds((lines, LANES), F32), 2, name="ffn_sum")(
        part, hidden_row.reshape(2 * lines, LANES)
    )
    summed = lax.all_gather(summed, "tp", axis=0, tiled=True)
    spread = kernel_call(final_norm_kernel, sds((SEQS, LANES), F32), 2, name="final_norm")(
        summed, gain_out.reshape(2 * lines, LANES)
    )
    spread = lax.all_to_all(spread.reshape(SEQS, 1, LANES), KV, 0, 0, tiled=True)
    layer_out = kernel_call(place_kernel, sds((cols, SEQS), BF16), 1, name="place")(
        spread.reshape(SEQS, LANES)
    )
    return (layer_out.T, new_state)


def solution(mesh):
    finer = Mesh(
        mesh.devices.reshape(mesh.shape["dp"], NZ, NY, mesh.shape["tp"]),
        ("dp", "kv_0", "kv_1", "tp"),
    )
    return jax.shard_map(
        on_device,
        mesh=finer,
        in_specs=(
            P("dp", KV),
            P(DP_KV),
            P(DP_KV, "tp", None, None),
            P(KV, "tp"),
            P(KV, "tp"),
            P(KV, "tp"),
            P(KV, "tp"),
            P(None, KV_TP),
            P(),
            P(None, KV_TP),
            P(None, KV_TP),
            P(KV_TP, None),
            P(),
        ),
        out_specs=(P("dp", KV_TP), P(DP_KV, "tp", None, None)),
        check_vma=False,
    )
```

```python
import jax
import jax.numpy as jnp
from jax import lax
from jax.experimental import pallas as pl
from jax.experimental.pallas import tpu as pltpu
from jax.sharding import Mesh
from jax.sharding import PartitionSpec as P

KV = ("kv_0", "kv_1")
YZ = ("kv_1", "kv_0")
KV_TP = ("kv_0", "kv_1", "tp")
DP_KV = ("dp", "kv_0", "kv_1")
F32 = jnp.float32
BF16 = jnp.bfloat16
LANES = 128
NZ = 16
NY = 4
SEQS = NZ * NY
INTERPRET = False

VMEM = pl.BlockSpec(memory_space=pltpu.VMEM)
PARAMS = pltpu.CompilerParams(vmem_limit_bytes=32 * 1024 * 1024)


def kernel_call(body, out_shape, n_in, scratch=(), name=None):
    single = not isinstance(out_shape, (list, tuple))
    return pl.pallas_call(
        body,
        out_shape=out_shape,
        in_specs=[VMEM] * n_in,
        out_specs=VMEM if single else [VMEM] * len(out_shape),
        scratch_shapes=list(scratch),
        compiler_params=PARAMS,
        interpret=INTERPRET,
        name=name,
    )


def sds(shape, dtype):
    return jax.ShapeDtypeStruct(shape, dtype)


def rows_of(s):
    return (s % NY) * NZ + s // NY


def perm_matrix(dtype):
    d = lax.broadcasted_iota(jnp.int32, (SEQS, SEQS), 0)
    s = lax.broadcasted_iota(jnp.int32, (SEQS, SEQS), 1)
    return (d == rows_of(s)).astype(F32).astype(dtype)


def mm(a, b, ca, cb):
    return lax.dot_general(a, b, (((ca,), (cb,)), ((), ())), preferred_element_type=F32)


def project_kernel(tok_hbm, wq, wk, wv, wg, out_hbm, tok, weights, out, sems, out_sems):
    sources = (wq, wk, wv, wg)
    count = len(sources)
    width = weights.shape[2]
    copies = [pltpu.make_async_copy(tok_hbm, tok, sems.at[count])]
    for i, w in enumerate(sources):
        copies.append(pltpu.make_async_copy(w, weights.at[i], sems.at[i]))
    for copy in copies:
        copy.start()
    copies[0].wait()
    rows = mm(perm_matrix(BF16), tok[...], 1, 0).astype(BF16)
    sends = []
    for i in range(count):
        copies[1 + i].wait()
        out[i] = mm(rows, weights[i], 1, 0).astype(BF16).reshape(NY, NZ, width)
        cols = pl.ds(i * width, width)
        sends.append(pltpu.make_async_copy(out.at[i], out_hbm.at[:, :, cols], out_sems.at[i]))
        sends[i].start()
    for send in sends:
        send.wait()


def near_sum_kernel(x, out, wide):
    for c in range(wide.shape[1]):
        cols = slice(c * LANES, (c + 1) * LANES)
        total = x[0, :, cols].astype(F32)
        for y in range(1, NY):
            total += x[y, :, cols].astype(F32)
        wide[:, c, :] = total
    out[...] = wide[...].astype(BF16)


def retention_kernel(x, aux, state, state_out, out, new_state, sems):
    heads, dim = state.shape[1], state.shape[2]
    total = x[0].astype(F32)
    for z in range(1, NZ):
        total += x[z].astype(F32)
    cosine = aux[0:1, :]
    sine = aux[1:2, :]
    query = total[0:heads]
    key = total[heads : 2 * heads]
    value = total[2 * heads : 3 * heads]
    gate = total[3 * heads : 4 * heads]
    query = query * cosine + pltpu.roll(query, dim // 2, 1) * sine
    key = (key * cosine + pltpu.roll(key, dim // 2, 1) * sine) * dim ** (-0.5)
    query_t = query.T
    key_t = key.T
    lines = []
    sends = []
    for h in range(heads):
        updated = aux[8 + h : 9 + h, :] * state[0, h] + key_t[:, h : h + 1] * value[h : h + 1, :]
        new_state[h] = updated
        sends.append(pltpu.make_async_copy(new_state.at[h], state_out.at[0, h], sems.at[h]))
        sends[h].start()
        lines.append(jnp.sum(query_t[:, h : h + 1] * updated, axis=0, keepdims=True))
    retained = jnp.concatenate(lines, axis=0)
    mean = jnp.mean(retained, -1, keepdims=True)
    var = jnp.mean(jnp.square(retained - mean), -1, keepdims=True)
    normed = (retained - mean) * lax.rsqrt(var + 1e-05)
    silu = gate / (1.0 + jnp.exp(-gate))
    attended = (normed * silu).astype(BF16)
    out[...] = jnp.broadcast_to(attended[None], out.shape)
    for send in sends:
        send.wait()


def mix_kernel(x, w_t, tok, out, wide):
    tp = lax.axis_index("tp")
    tps, seqs, heads, dim = x.shape
    cols = w_t.shape[0]
    groups = LANES // cols
    wide[...] = x[...].astype(F32)
    own = lax.broadcasted_iota(jnp.int32, (tok.shape[1], LANES), 0)
    lane = lax.broadcasted_iota(jnp.int32, (tok.shape[1], LANES), 1)
    pick = (own == tp * cols + lane % cols).astype(F32).astype(BF16)
    rows = mm(perm_matrix(BF16), tok[...], 1, 0).astype(BF16)
    acc = mm(rows, pick, 1, 0)
    w4 = jnp.concatenate([w_t[...]] * groups, axis=0)
    for t in range(tps):
        for h in range(heads):
            k = (t * heads + h) * dim
            acc += mm(wide[t, :, h, :].astype(BF16), w4[:, k : k + dim], 1, 1)
    block = lax.broadcasted_iota(jnp.int32, (seqs // groups, LANES), 1) // cols
    per = seqs // groups
    packed = acc[0:per]
    for g in range(1, groups):
        packed = jnp.where(block == g, acc[g * per : (g + 1) * per], packed)
    out[...] = jnp.broadcast_to(packed.astype(BF16)[None], out.shape)


def feed_kernel(x, gain, wg_t, wu_t, wd, own, other, row, wide, narrow, sums_out):
    tps = x.shape[0]
    per = x.shape[3]
    tp = lax.axis_index("tp")
    place = lax.axis_index("kv_1") * NZ + lax.axis_index("kv_0")
    groups = SEQS // per
    cols = LANES // groups
    chips = LANES // (tps * cols)
    width = wide.shape[1]
    lane = lax.broadcasted_iota(jnp.int32, (per, LANES), 1) // cols
    sums = [jnp.zeros((per, LANES), F32) for _ in range(groups)]
    squares = [jnp.zeros((per, LANES), F32) for _ in range(groups)]
    for a in range(SEQS // chips):
        tiles = [None] * groups
        for q in range(groups):
            kv = a * chips + q // tps
            source = x[q % tps, kv % NY, kv // NY].astype(F32)
            for g in range(groups):
                shift = ((q - g) * cols) % LANES
                moved = source if shift == 0 else pltpu.roll(source, shift, 1)
                tiles[g] = moved if q == 0 else jnp.where(lane == q, moved, tiles[g])
        for g in range(groups):
            wide[g * per : (g + 1) * per, a * LANES : (a + 1) * LANES] = tiles[g]
            sums[g] += tiles[g]
            squares[g] += tiles[g] * tiles[g]
    mean = jnp.sum(jnp.concatenate(sums, 0), -1, keepdims=True) / width
    var = jnp.sum(jnp.concatenate(squares, 0), -1, keepdims=True) / width - mean * mean
    scale = lax.rsqrt(var + 1e-05)
    for a in range(width // LANES):
        c = slice(a * LANES, (a + 1) * LANES)
        hidden = ((wide[:, c] - mean) * scale * gain[:, c]).astype(BF16)
        narrow[:, c] = hidden
        wide[:, c] = hidden.astype(F32)
    row[...] = wide[pl.ds(place, 1), :]
    gate = mm(narrow[...], wg_t[...], 1, 1)
    up = mm(narrow[...], wu_t[...], 1, 1)
    inner = (gate / (1.0 + jnp.exp(-gate)) * up).astype(BF16)
    half = own.shape[1]
    step = 4
    for t in range(tps):
        for c in range(0, half, step):
            k = (t * half + c) * LANES
            part = mm(inner, wd[:, k : k + step * LANES], 1, 0)
            for i in range(step):
                sums_out[t, :, c + i, :] = part[:, i * LANES : (i + 1) * LANES]
    own[...] = sums_out[tp].astype(BF16)
    other[...] = sums_out[1 - tp].astype(BF16)


def pair_sum_kernel(own, both, out):
    tp = lax.axis_index("tp")
    out[...] = (own[...].astype(F32) + both[1 - tp].astype(F32)).astype(BF16)


def plain_sum_kernel(x, out):
    total = x[0].astype(F32)
    for d in range(1, x.shape[0]):
        total += x[d].astype(F32)
    out[...] = total.astype(BF16)


def ffn_sum_kernel(x, hidden, out):
    per = x.shape[1]
    tp = lax.axis_index("tp")
    total = hidden[pl.ds(pl.multiple_of(tp * per, per), per), :]
    for d in range(x.shape[0]):
        total += x[d].astype(F32)
    out[...] = total


def total_of(x):
    return jnp.sum(jnp.sum(x, 0, keepdims=True), 1, keepdims=True)


def final_norm_kernel(x, gain, out):
    p = x[...]
    count = p.shape[0] * p.shape[1]
    mean = total_of(p) / count
    var = total_of(p * p) / count - mean * mean
    normed = ((p - mean) * lax.rsqrt(var + 1e-05) * gain[...]).astype(BF16)
    lines = p.shape[0]
    d = lax.broadcasted_iota(jnp.int32, (SEQS, lines), 0)
    line = lax.broadcasted_iota(jnp.int32, (SEQS, lines), 1)
    spread = (d * lines // SEQS == line).astype(F32).astype(BF16)
    out[...] = mm(spread, normed, 1, 0)


def place_kernel(x, out):
    cols = out.shape[0]
    offset = (lax.axis_index("kv_1") % 2) * (2 * cols) + lax.axis_index("tp") * cols
    col = lax.broadcasted_iota(jnp.int32, (cols, LANES), 0)
    lane = lax.broadcasted_iota(jnp.int32, (cols, LANES), 1)
    pick = (lane == col + offset).astype(F32).astype(BF16)
    out[...] = mm(pick, x[...].astype(BF16), 1, 1).astype(BF16)


def on_device(
    tokens,
    positions,
    state,
    w_query,
    w_key,
    w_value,
    w_gate,
    w_out,
    gain_mix,
    w_ffn_gate,
    w_ffn_up,
    w_ffn_down,
    gain_out,
):
    heads, dim = state.shape[1], state.shape[2]
    width = w_ffn_gate.shape[0]
    cols = w_out.shape[1]
    proj = 4 * heads
    half = width // 2
    tp = lax.axis_index("tp")

    inverse = 10000.0 ** (-jnp.arange(dim // 2, dtype=F32) / (dim // 2))
    angle = positions.astype(F32)[:, None] * inverse[None, :]
    cosine = jnp.cos(angle)
    sine = jnp.sin(angle)
    head_ids = (tp * heads + jnp.arange(heads, dtype=jnp.int32)).astype(F32)
    decay = 1.0 - 2.0 ** (-5.0 - 6.0 * head_ids / (2 * heads - 1))
    aux = jnp.concatenate(
        [
            jnp.concatenate([cosine, cosine], 1),
            jnp.concatenate([-sine, sine], 1),
            jnp.zeros((6, dim), F32),
            jnp.broadcast_to(decay[:, None], (heads, dim)),
        ],
        0,
    )

    tokens_in, aux = lax.optimization_barrier((tokens, aux))
    parts = pl.pallas_call(
        project_kernel,
        out_shape=sds((NY, NZ, proj * dim), BF16),
        in_specs=[pl.BlockSpec(memory_space=pl.ANY)] * 5,
        out_specs=pl.BlockSpec(memory_space=pl.ANY),
        scratch_shapes=[
            pltpu.VMEM(tokens.shape, BF16),
            pltpu.VMEM((4, *w_query.shape), BF16),
            pltpu.VMEM((4, NY, NZ, w_query.shape[1]), BF16),
            pltpu.SemaphoreType.DMA((5,)),
            pltpu.SemaphoreType.DMA((4,)),
        ],
        interpret=INTERPRET,
        name="project",
    )(tokens_in, w_query, w_key, w_value, w_gate)
    near = lax.all_to_all(parts, "kv_1", 0, 0, tiled=True)
    near = kernel_call(
        near_sum_kernel,
        sds((NZ, proj, dim), BF16),
        1,
        scratch=[pltpu.VMEM((NZ, proj, dim), F32)],
        name="near_sum",
    )(near)
    far = lax.all_to_all(near, "kv_0", 0, 0, tiled=True)
    new_state, attended = pl.pallas_call(
        retention_kernel,
        out_shape=[sds(state.shape, F32), sds((SEQS, heads, dim), BF16)],
        in_specs=[VMEM] * 3,
        out_specs=[pl.BlockSpec(memory_space=pl.ANY), VMEM],
        scratch_shapes=[pltpu.VMEM(state.shape[1:], F32), pltpu.SemaphoreType.DMA((heads,))],
        compiler_params=PARAMS,
        interpret=INTERPRET,
        name="retention",
    )(far, aux, state)
    gathered = lax.all_to_all(attended, YZ, 0, 0, tiled=True)
    gathered = lax.all_gather(gathered, "tp", axis=0)
    per = SEQS * cols // LANES
    mixed = kernel_call(
        mix_kernel,
        sds((NZ, per, LANES), BF16),
        3,
        scratch=[pltpu.VMEM((2, SEQS, heads, dim), F32)],
        name="mix",
    )(gathered.reshape(2, SEQS, heads, dim), w_out.T, tokens)
    rows = lax.all_to_all(mixed, "kv_0", 0, 0, tiled=True)
    rows = jnp.broadcast_to(rows[None], (NY, *rows.shape))
    rows = lax.all_to_all(rows, "kv_1", 0, 0, tiled=True)
    rows = lax.all_gather(rows, "tp", axis=0)
    lines = half // LANES
    own, other, hidden_row = kernel_call(
        feed_kernel,
        [sds((SEQS, lines, LANES), BF16)] * 2 + [sds((1, width), F32)],
        5,
        scratch=[
            pltpu.VMEM((SEQS, width), F32),
            pltpu.VMEM((SEQS, width), BF16),
            pltpu.VMEM((2, SEQS, lines, LANES), F32),
        ],
        name="feed",
    )(rows, gain_mix[None, :], w_ffn_gate.T, w_ffn_up.T, w_ffn_down)
    both = lax.all_gather(other, "tp", axis=0)
    part = kernel_call(pair_sum_kernel, sds(own.shape, BF16), 2, name="pair_sum")(own, both)
    part = part.reshape(NY, NZ, lines, LANES)
    part = lax.all_to_all(part, "kv_1", 0, 0, tiled=True)
    part = kernel_call(plain_sum_kernel, sds((NZ, lines, LANES), BF16), 1, name="half_sum")(part)
    part = lax.all_to_all(part, "kv_0", 0, 0, tiled=True)
    summed = kernel_call(ffn_sum_kernel, sds((lines, LANES), F32), 2, name="ffn_sum")(
        part, hidden_row.reshape(2 * lines, LANES)
    )
    summed = lax.all_gather(summed, "tp", axis=0, tiled=True)
    spread = kernel_call(final_norm_kernel, sds((SEQS, LANES), F32), 2, name="final_norm")(
        summed, gain_out.reshape(2 * lines, LANES)
    )
    spread = lax.all_to_all(spread.reshape(SEQS, 1, LANES), KV, 0, 0, tiled=True)
    layer_out = kernel_call(place_kernel, sds((cols, SEQS), BF16), 1, name="place")(
        spread.reshape(SEQS, LANES)
    )
    return (layer_out.T, new_state)


def solution(mesh):
    finer = Mesh(
        mesh.devices.reshape(mesh.shape["dp"], NZ, NY, mesh.shape["tp"]),
        ("dp", "kv_0", "kv_1", "tp"),
    )
    return jax.shard_map(
        on_device,
        mesh=finer,
        in_specs=(
            P("dp", KV),
            P(DP_KV),
            P(DP_KV, "tp", None, None),
            P(KV, "tp"),
            P(KV, "tp"),
            P(KV, "tp"),
            P(KV, "tp"),
            P(None, KV_TP),
            P(),
            P(None, KV_TP),
            P(None, KV_TP),
            P(KV_TP, None),
            P(),
        ),
        out_specs=(P("dp", KV_TP), P(DP_KV, "tp", None, None)),
        check_vma=False,
    )
```

```python
import jax
import jax.numpy as jnp
from jax import lax
from jax.experimental import pallas as pl
from jax.experimental.pallas import tpu as pltpu
from jax.sharding import Mesh
from jax.sharding import PartitionSpec as P

KV = ("kv_0", "kv_1")
YZ = ("kv_1", "kv_0")
KV_TP = ("kv_0", "kv_1", "tp")
DP_KV = ("dp", "kv_0", "kv_1")
F32 = jnp.float32
BF16 = jnp.bfloat16
LANES = 128
NZ = 16
NY = 4
SEQS = NZ * NY
INTERPRET = False

VMEM = pl.BlockSpec(memory_space=pltpu.VMEM)
PARAMS = pltpu.CompilerParams(vmem_limit_bytes=32 * 1024 * 1024)


def kernel_call(body, out_shape, n_in, scratch=(), name=None):
    single = not isinstance(out_shape, (list, tuple))
    return pl.pallas_call(
        body,
        out_shape=out_shape,
        in_specs=[VMEM] * n_in,
        out_specs=VMEM if single else [VMEM] * len(out_shape),
        scratch_shapes=list(scratch),
        compiler_params=PARAMS,
        interpret=INTERPRET,
        name=name,
    )


def sds(shape, dtype):
    return jax.ShapeDtypeStruct(shape, dtype)


def rows_of(s):
    return (s % NY) * NZ + s // NY


def perm_matrix(dtype):
    d = lax.broadcasted_iota(jnp.int32, (SEQS, SEQS), 0)
    s = lax.broadcasted_iota(jnp.int32, (SEQS, SEQS), 1)
    return (d == rows_of(s)).astype(F32).astype(dtype)


def mm(a, b, ca, cb):
    return lax.dot_general(a, b, (((ca,), (cb,)), ((), ())), preferred_element_type=F32)


def project_kernel(tok_hbm, wq, wk, wv, wg, out_hbm, tok, weights, out, sems, out_sems):
    sources = (wq, wk, wv, wg)
    count = len(sources)
    width = weights.shape[2]
    copies = [pltpu.make_async_copy(tok_hbm, tok, sems.at[count])]
    for i, w in enumerate(sources):
        copies.append(pltpu.make_async_copy(w, weights.at[i], sems.at[i]))
    for copy in copies:
        copy.start()
    copies[0].wait()
    rows = mm(perm_matrix(BF16), tok[...], 1, 0).astype(BF16)
    sends = []
    for i in range(count):
        copies[1 + i].wait()
        out[i] = mm(rows, weights[i], 1, 0).astype(BF16).reshape(NY, NZ, width)
        cols = pl.ds(i * width, width)
        sends.append(pltpu.make_async_copy(out.at[i], out_hbm.at[:, :, cols], out_sems.at[i]))
        sends[i].start()
    for send in sends:
        send.wait()


def near_sum_kernel(x, out, wide):
    for c in range(wide.shape[1]):
        cols = slice(c * LANES, (c + 1) * LANES)
        total = x[0, :, cols].astype(F32)
        for y in range(1, NY):
            total += x[y, :, cols].astype(F32)
        wide[:, c, :] = total
    out[...] = wide[...].astype(BF16)


def retention_kernel(x, aux, state, state_out, out, new_state, sems):
    heads, dim = state.shape[1], state.shape[2]
    total = x[0].astype(F32)
    for z in range(1, NZ):
        total += x[z].astype(F32)
    cosine = aux[0:1, :]
    sine = aux[1:2, :]
    query = total[0:heads]
    key = total[heads : 2 * heads]
    value = total[2 * heads : 3 * heads]
    gate = total[3 * heads : 4 * heads]
    query = query * cosine + pltpu.roll(query, dim // 2, 1) * sine
    key = (key * cosine + pltpu.roll(key, dim // 2, 1) * sine) * dim ** (-0.5)
    query_t = query.T
    key_t = key.T
    lines = []
    sends = []
    for h in range(heads):
        updated = aux[8 + h : 9 + h, :] * state[0, h] + key_t[:, h : h + 1] * value[h : h + 1, :]
        new_state[h] = updated
        sends.append(pltpu.make_async_copy(new_state.at[h], state_out.at[0, h], sems.at[h]))
        sends[h].start()
        lines.append(jnp.sum(query_t[:, h : h + 1] * updated, axis=0, keepdims=True))
    retained = jnp.concatenate(lines, axis=0)
    mean = jnp.mean(retained, -1, keepdims=True)
    var = jnp.mean(jnp.square(retained - mean), -1, keepdims=True)
    normed = (retained - mean) * lax.rsqrt(var + 1e-05)
    silu = gate / (1.0 + jnp.exp(-gate))
    attended = (normed * silu).astype(BF16)
    out[...] = jnp.broadcast_to(attended[None], out.shape)
    for send in sends:
        send.wait()


def mix_kernel(x, w_t, tok, out, wide):
    tp = lax.axis_index("tp")
    tps, seqs, heads, dim = x.shape
    cols = w_t.shape[0]
    groups = LANES // cols
    wide[...] = x[...].astype(F32)
    own = lax.broadcasted_iota(jnp.int32, (tok.shape[1], LANES), 0)
    lane = lax.broadcasted_iota(jnp.int32, (tok.shape[1], LANES), 1)
    pick = (own == tp * cols + lane % cols).astype(F32).astype(BF16)
    rows = mm(perm_matrix(BF16), tok[...], 1, 0).astype(BF16)
    acc = mm(rows, pick, 1, 0)
    w4 = jnp.concatenate([w_t[...]] * groups, axis=0)
    for t in range(tps):
        for h in range(heads):
            k = (t * heads + h) * dim
            acc += mm(wide[t, :, h, :].astype(BF16), w4[:, k : k + dim], 1, 1)
    per = seqs // groups
    turn = (lax.axis_index("kv_1") % (groups // tps)) * tps + tp
    block = lax.broadcasted_iota(jnp.int32, (per, LANES), 1) // cols
    block = (block + groups - turn) % groups
    packed = acc[0:per]
    for g in range(1, groups):
        packed = jnp.where(block == g, acc[g * per : (g + 1) * per], packed)
    out[...] = jnp.broadcast_to(packed.astype(BF16)[None], out.shape)


def feed_kernel(x, gain, wg_t, wu_t, wd, own, other, row, wide, narrow, stats):
    tps = x.shape[0]
    per = x.shape[3]
    tp = lax.axis_index("tp")
    place = lax.axis_index("kv_1") * NZ + lax.axis_index("kv_0")
    groups = SEQS // per
    cols = LANES // groups
    chips = groups // tps
    width = wide.shape[1]
    lane = lax.broadcasted_iota(jnp.int32, (per, LANES), 1) // cols
    sums = [jnp.zeros((per, LANES), F32) for _ in range(groups)]
    squares = [jnp.zeros((per, LANES), F32) for _ in range(groups)]
    for a in range(SEQS // chips):
        sources = []
        for q in range(groups):
            kv = a * chips + q // tps
            sources.append(x[q % tps, kv % NY, kv // NY].astype(F32))
        for g in range(groups):
            tile = sources[(groups - g) % groups]
            for j in range(1, groups):
                tile = jnp.where(lane == j, sources[(j - g) % groups], tile)
            if g:
                tile = pltpu.roll(tile, LANES - g * cols, 1)
            wide[g * per : (g + 1) * per, a * LANES : (a + 1) * LANES] = tile
            sums[g] += tile
            squares[g] += tile * tile
    mean = jnp.sum(jnp.concatenate(sums, 0), -1, keepdims=True) / width
    var = jnp.sum(jnp.concatenate(squares, 0), -1, keepdims=True) / width - mean * mean
    scale = lax.rsqrt(var + 1e-05)
    stats[0] = jnp.broadcast_to(mean, stats.shape[1:])
    stats[1] = jnp.broadcast_to(scale, stats.shape[1:])
    for a in range(width // LANES):
        c = slice(a * LANES, (a + 1) * LANES)
        narrow[:, c] = ((wide[:, c] - mean) * scale * gain[:, c]).astype(BF16)
    own_mean = stats[0, pl.ds(place, 1), 0:1]
    own_scale = stats[1, pl.ds(place, 1), 0:1]
    own_row = (wide[pl.ds(place, 1), :] - own_mean) * own_scale * gain[...]
    row[...] = own_row.astype(BF16).astype(F32)
    gate = mm(narrow[...], wg_t[...], 1, 1)
    up = mm(narrow[...], wu_t[...], 1, 1)
    inner = (gate / (1.0 + jnp.exp(-gate)) * up).astype(BF16)
    half = own.shape[1]
    step = 4 * LANES
    for c in range(0, half, step):
        mine = pl.multiple_of(tp * half + c, step)
        theirs = pl.multiple_of((1 - tp) * half + c, step)
        own[:, c : c + step] = mm(inner, wd[:, pl.ds(mine, step)], 1, 0).astype(BF16)
        other[:, c : c + step] = mm(inner, wd[:, pl.ds(theirs, step)], 1, 0).astype(BF16)


def pair_sum_kernel(own, both, out):
    tp = lax.axis_index("tp")
    out[...] = (own[...].astype(F32) + both[1 - tp].astype(F32)).astype(BF16)


def ffn_sum_kernel(x, hidden, out):
    per = x.shape[1]
    tp = lax.axis_index("tp")
    total = hidden[pl.ds(pl.multiple_of(tp * per, per), per), :]
    for d in range(x.shape[0]):
        total += x[d].astype(F32)
    out[...] = total


def total_of(x):
    return jnp.sum(jnp.sum(x, 0, keepdims=True), 1, keepdims=True)


def final_norm_kernel(x, gain, out):
    p = x[...]
    count = p.shape[0] * p.shape[1]
    mean = total_of(p) / count
    var = total_of(p * p) / count - mean * mean
    normed = ((p - mean) * lax.rsqrt(var + 1e-05) * gain[...]).astype(BF16)
    lines = p.shape[0]
    d = lax.broadcasted_iota(jnp.int32, (SEQS, lines), 0)
    line = lax.broadcasted_iota(jnp.int32, (SEQS, lines), 1)
    spread = (d * lines // SEQS == line).astype(F32).astype(BF16)
    out[...] = mm(spread, normed, 1, 0)


def place_kernel(x, out):
    cols = out.shape[0]
    offset = (lax.axis_index("kv_1") % 2) * (2 * cols) + lax.axis_index("tp") * cols
    col = lax.broadcasted_iota(jnp.int32, (cols, LANES), 0)
    lane = lax.broadcasted_iota(jnp.int32, (cols, LANES), 1)
    pick = (lane == col + offset).astype(F32).astype(BF16)
    out[...] = mm(pick, x[...].astype(BF16), 1, 1).astype(BF16)


def on_device(
    tokens,
    positions,
    state,
    w_query,
    w_key,
    w_value,
    w_gate,
    w_out,
    gain_mix,
    w_ffn_gate,
    w_ffn_up,
    w_ffn_down,
    gain_out,
):
    heads, dim = state.shape[1], state.shape[2]
    width = w_ffn_gate.shape[0]
    cols = w_out.shape[1]
    proj = 4 * heads
    half = width // 2
    tp = lax.axis_index("tp")

    inverse = 10000.0 ** (-jnp.arange(dim // 2, dtype=F32) / (dim // 2))
    angle = positions.astype(F32)[:, None] * inverse[None, :]
    cosine = jnp.cos(angle)
    sine = jnp.sin(angle)
    head_ids = (tp * heads + jnp.arange(heads, dtype=jnp.int32)).astype(F32)
    decay = 1.0 - 2.0 ** (-5.0 - 6.0 * head_ids / (2 * heads - 1))
    aux = jnp.concatenate(
        [
            jnp.concatenate([cosine, cosine], 1),
            jnp.concatenate([-sine, sine], 1),
            jnp.zeros((6, dim), F32),
            jnp.broadcast_to(decay[:, None], (heads, dim)),
        ],
        0,
    )

    tokens_in, aux = lax.optimization_barrier((tokens, aux))
    parts = pl.pallas_call(
        project_kernel,
        out_shape=sds((NY, NZ, proj * dim), BF16),
        in_specs=[pl.BlockSpec(memory_space=pl.ANY)] * 5,
        out_specs=pl.BlockSpec(memory_space=pl.ANY),
        scratch_shapes=[
            pltpu.VMEM(tokens.shape, BF16),
            pltpu.VMEM((4, *w_query.shape), BF16),
            pltpu.VMEM((4, NY, NZ, w_query.shape[1]), BF16),
            pltpu.SemaphoreType.DMA((5,)),
            pltpu.SemaphoreType.DMA((4,)),
        ],
        interpret=INTERPRET,
        name="project",
    )(tokens_in, w_query, w_key, w_value, w_gate)
    near = lax.all_to_all(parts, "kv_1", 0, 0, tiled=True)
    near = kernel_call(
        near_sum_kernel,
        sds((NZ, proj, dim), BF16),
        1,
        scratch=[pltpu.VMEM((NZ, proj, dim), F32)],
        name="near_sum",
    )(near)
    far = lax.all_to_all(near, "kv_0", 0, 0, tiled=True)
    new_state, attended = pl.pallas_call(
        retention_kernel,
        out_shape=[sds(state.shape, F32), sds((SEQS, heads, dim), BF16)],
        in_specs=[VMEM] * 3,
        out_specs=[pl.BlockSpec(memory_space=pl.ANY), VMEM],
        scratch_shapes=[pltpu.VMEM(state.shape[1:], F32), pltpu.SemaphoreType.DMA((heads,))],
        compiler_params=PARAMS,
        interpret=INTERPRET,
        name="retention",
    )(far, aux, state)
    gathered = lax.all_to_all(attended, YZ, 0, 0, tiled=True)
    gathered = lax.all_gather(gathered, "tp", axis=0)
    per = SEQS * cols // LANES
    mixed = kernel_call(
        mix_kernel,
        sds((NZ, per, LANES), BF16),
        3,
        scratch=[pltpu.VMEM((2, SEQS, heads, dim), F32)],
        name="mix",
    )(gathered.reshape(2, SEQS, heads, dim), w_out.T, tokens)
    rows = lax.all_to_all(mixed, "kv_0", 0, 0, tiled=True)
    rows = jnp.broadcast_to(rows[None], (NY, *rows.shape))
    rows = lax.all_to_all(rows, "kv_1", 0, 0, tiled=True)
    rows = lax.all_gather(rows, "tp", axis=0)
    lines = half // LANES
    own, other, hidden_row = kernel_call(
        feed_kernel,
        [sds((SEQS, half), BF16)] * 2 + [sds((1, width), F32)],
        5,
        scratch=[
            pltpu.VMEM((SEQS, width), F32),
            pltpu.VMEM((SEQS, width), BF16),
            pltpu.VMEM((2, SEQS, LANES), F32),
        ],
        name="feed",
    )(rows, gain_mix[None, :], w_ffn_gate.T, w_ffn_up.T, w_ffn_down)
    both = lax.all_gather(other, "tp", axis=0)
    part = kernel_call(pair_sum_kernel, sds(own.shape, BF16), 2, name="pair_sum")(own, both)
    part = lax.all_to_all(part.reshape(NY, NZ, half), "kv_1", 0, 0, tiled=True)
    part = kernel_call(
        near_sum_kernel,
        sds((NZ, lines, LANES), BF16),
        1,
        scratch=[pltpu.VMEM((NZ, lines, LANES), F32)],
        name="half_sum",
    )(part)
    part = lax.all_to_all(part, "kv_0", 0, 0, tiled=True)
    summed = kernel_call(ffn_sum_kernel, sds((lines, LANES), F32), 2, name="ffn_sum")(
        part, hidden_row.reshape(2 * lines, LANES)
    )
    summed = lax.all_gather(summed, "tp", axis=0, tiled=True)
    spread = kernel_call(final_norm_kernel, sds((SEQS, LANES), F32), 2, name="final_norm")(
        summed, gain_out.reshape(2 * lines, LANES)
    )
    spread = lax.all_to_all(spread.reshape(SEQS, 1, LANES), KV, 0, 0, tiled=True)
    layer_out = kernel_call(place_kernel, sds((cols, SEQS), BF16), 1, name="place")(
        spread.reshape(SEQS, LANES)
    )
    return (layer_out.T, new_state)


def solution(mesh):
    finer = Mesh(
        mesh.devices.reshape(mesh.shape["dp"], NZ, NY, mesh.shape["tp"]),
        ("dp", "kv_0", "kv_1", "tp"),
    )
    return jax.shard_map(
        on_device,
        mesh=finer,
        in_specs=(
            P("dp", KV),
            P(DP_KV),
            P(DP_KV, "tp", None, None),
            P(KV, "tp"),
            P(KV, "tp"),
            P(KV, "tp"),
            P(KV, "tp"),
            P(None, KV_TP),
            P(),
            P(None, KV_TP),
            P(None, KV_TP),
            P(KV_TP, None),
            P(),
        ),
        out_specs=(P("dp", KV_TP), P(DP_KV, "tp", None, None)),
        check_vma=False,
    )
```

```python
import jax
import jax.numpy as jnp
from jax import lax
from jax.experimental import pallas as pl
from jax.experimental.pallas import tpu as pltpu
from jax.sharding import Mesh
from jax.sharding import PartitionSpec as P

KV = ("kv_0", "kv_1")
KV_TP = ("kv_0", "kv_1", "tp")
DP_KV = ("dp", "kv_0", "kv_1")
F32 = jnp.float32
BF16 = jnp.bfloat16
LANES = 128
NZ = 16
NY = 4
SEQS = NZ * NY
ORDER_0 = (0, 3, 1, 2)
ORDER_1 = (2, 0, 3, 1)
INTERPRET = False

VMEM = pl.BlockSpec(memory_space=pltpu.VMEM)
PARAMS = pltpu.CompilerParams(vmem_limit_bytes=32 * 1024 * 1024)


def kernel_call(body, out_shape, n_in, scratch=(), name=None):
    single = not isinstance(out_shape, (list, tuple))
    return pl.pallas_call(
        body,
        out_shape=out_shape,
        in_specs=[VMEM] * n_in,
        out_specs=VMEM if single else [VMEM] * len(out_shape),
        scratch_shapes=list(scratch),
        compiler_params=PARAMS,
        interpret=INTERPRET,
        name=name,
    )


def sds(shape, dtype):
    return jax.ShapeDtypeStruct(shape, dtype)


def rows_of(s):
    return (s % NY) * NZ + s // NY


def perm_matrix(dtype):
    d = lax.broadcasted_iota(jnp.int32, (SEQS, SEQS), 0)
    s = lax.broadcasted_iota(jnp.int32, (SEQS, SEQS), 1)
    return (d == rows_of(s)).astype(F32).astype(dtype)


def mm(a, b, ca, cb):
    return lax.dot_general(a, b, (((ca,), (cb,)), ((), ())), preferred_element_type=F32)


def project_kernel(
    tok_hbm, wq, wk, wv, wg, w_out, out_hbm, tok, weights, out, residual, sems, out_sems, share_sems
):
    sources = (wq, wk, wv, wg)
    count = len(sources)
    width = weights.shape[2]
    copies = [pltpu.make_async_copy(tok_hbm, tok, sems.at[count])]
    for i, w in enumerate(sources):
        copies.append(pltpu.make_async_copy(w, weights.at[i], sems.at[i]))
    for copy in copies:
        copy.start()
    sends = []
    depth = w_out.shape[1]
    for part in range(w_out.shape[0] // NZ):
        cols = pl.ds(count * width + part * depth, depth)
        for y in range(NY):
            sends.append(
                pltpu.make_async_copy(
                    w_out.at[pl.ds(part * NZ, NZ)], out_hbm.at[y, :, cols], share_sems.at[part, y]
                )
            )
            sends[-1].start()
    copies[0].wait()
    rows = mm(perm_matrix(BF16), tok[...], 1, 0).astype(BF16)
    residual[...] = jnp.zeros(residual.shape, BF16)
    for y in range(NY):
        residual[y, :, 0 : rows.shape[1]] = rows[y * NZ : (y + 1) * NZ]
    tail = pl.ds(out_hbm.shape[2] - LANES, LANES)
    sends.append(pltpu.make_async_copy(residual, out_hbm.at[:, :, tail], out_sems.at[count]))
    sends[-1].start()
    for i in range(count):
        copies[1 + i].wait()
        out[i] = mm(rows, weights[i], 1, 0).astype(BF16).reshape(NY, NZ, width)
        cols = pl.ds(i * width, width)
        sends.append(pltpu.make_async_copy(out.at[i], out_hbm.at[:, :, cols], out_sems.at[i]))
        sends[-1].start()
    for send in sends:
        send.wait()


def near_sum_kernel(x, out, wide):
    for c in range(wide.shape[1]):
        cols = slice(c * LANES, (c + 1) * LANES)
        total = x[0, :, cols].astype(F32)
        for y in range(1, NY):
            total += x[y, :, cols].astype(F32)
        wide[:, c, :] = total
    out[...] = wide[...].astype(BF16)


def retention_kernel(x, aux, state, state_out, out, new_state, sems):
    heads, dim = state.shape[1], state.shape[2]
    total = x[0].astype(F32)
    for z in range(1, NZ):
        total += x[z].astype(F32)
    cosine = aux[0:1, :]
    sine = aux[1:2, :]
    query = total[0:heads]
    key = total[heads : 2 * heads]
    value = total[2 * heads : 3 * heads]
    gate = total[3 * heads : 4 * heads]
    query = query * cosine + pltpu.roll(query, dim // 2, 1) * sine
    key = (key * cosine + pltpu.roll(key, dim // 2, 1) * sine) * dim ** (-0.5)
    query_t = query.T
    key_t = key.T
    lines = []
    sends = []
    for h in range(heads):
        updated = aux[8 + h : 9 + h, :] * state[0, h] + key_t[:, h : h + 1] * value[h : h + 1, :]
        new_state[h] = updated
        sends.append(pltpu.make_async_copy(new_state.at[h], state_out.at[0, h], sems.at[h]))
        sends[h].start()
        lines.append(jnp.sum(query_t[:, h : h + 1] * updated, axis=0, keepdims=True))
    retained = jnp.concatenate(lines, axis=0)
    mean = jnp.mean(retained, -1, keepdims=True)
    var = jnp.mean(jnp.square(retained - mean), -1, keepdims=True)
    normed = (retained - mean) * lax.rsqrt(var + 1e-05)
    silu = gate / (1.0 + jnp.exp(-gate))
    attended = (normed * silu).astype(BF16)
    out[...] = jnp.broadcast_to(attended[None], out.shape)
    for send in sends:
        send.wait()


def mix_kernel(x, shared, out, wide):
    tp = lax.axis_index("tp")
    tps, _, heads, dim = x.shape
    cols = LANES // NY
    depth = tps * heads * dim
    first = shared.shape[2] - LANES - 2 * depth
    wide[...] = x[...].astype(F32)
    owners = [jnp.where(tp == 0, even, odd) for even, odd in zip(ORDER_0, ORDER_1)]
    own = lax.broadcasted_iota(jnp.int32, (LANES, LANES), 0)
    lane = lax.broadcasted_iota(jnp.int32, (LANES, LANES), 1)
    acc = jnp.zeros((NZ, LANES), F32)
    for b, y in enumerate(owners):
        pick = (own == tp * cols + lane % cols) & (lane // cols == b)
        pick = pick.astype(F32).astype(BF16)
        acc += mm(shared[y, :, first + 2 * depth :], pick, 1, 0)
    for t in range(tps):
        for h in range(heads):
            k = first + (t * heads + h) * dim
            pieces = []
            for y in owners:
                pieces.append(shared[y, :, k : k + dim])
                pieces.append(shared[y, :, k + depth : k + depth + dim])
            weight = jnp.concatenate(pieces, axis=0)
            acc += mm(wide[t, :, h, :].astype(BF16), weight, 1, 1)
    out[...] = jnp.broadcast_to(acc.astype(BF16)[None], out.shape)


def feed_kernel(x, gain, wg_t, wu_t, wd, own, other, row, wide, narrow, stats):
    per = x.shape[3]
    tp = lax.axis_index("tp")
    place = lax.axis_index("kv_1") * NZ + lax.axis_index("kv_0")
    cols = LANES // NY
    width = wide.shape[1]
    odd = (lax.broadcasted_iota(jnp.int32, (per, LANES), 1) // cols) % 2 == 1
    sums = [jnp.zeros((per, LANES), F32) for _ in range(NY)]
    squares = [jnp.zeros((per, LANES), F32) for _ in range(NY)]
    for z in range(NZ):
        for y in range(NY):
            a = x[0, y, z].astype(F32)
            b = x[1, y, z].astype(F32)
            low = jnp.where(odd, b, a)
            high = pltpu.roll(jnp.where(odd, a, b), cols, 1)
            wide[y * per : (y + 1) * per, 2 * z * LANES : (2 * z + 1) * LANES] = low
            wide[y * per : (y + 1) * per, (2 * z + 1) * LANES : (2 * z + 2) * LANES] = high
            sums[y] += low + high
            squares[y] += low * low + high * high
    mean = jnp.sum(jnp.concatenate(sums, 0), -1, keepdims=True) / width
    var = jnp.sum(jnp.concatenate(squares, 0), -1, keepdims=True) / width - mean * mean
    scale = lax.rsqrt(var + 1e-05)
    stats[0] = jnp.broadcast_to(mean, stats.shape[1:])
    stats[1] = jnp.broadcast_to(scale, stats.shape[1:])
    for a in range(width // LANES):
        c = slice(a * LANES, (a + 1) * LANES)
        narrow[:, c] = ((wide[:, c] - mean) * scale * gain[:, c]).astype(BF16)
    own_mean = stats[0, pl.ds(place, 1), 0:1]
    own_scale = stats[1, pl.ds(place, 1), 0:1]
    own_row = (wide[pl.ds(place, 1), :] - own_mean) * own_scale * gain[...]
    row[...] = own_row.astype(BF16).astype(F32)
    gate = mm(narrow[...], wg_t[...], 1, 1)
    up = mm(narrow[...], wu_t[...], 1, 1)
    inner = (gate / (1.0 + jnp.exp(-gate)) * up).astype(BF16)
    half = own.shape[1]
    step = 4 * LANES
    for c in range(0, half, step):
        mine = pl.multiple_of(tp * half + c, step)
        theirs = pl.multiple_of((1 - tp) * half + c, step)
        own[:, c : c + step] = mm(inner, wd[:, pl.ds(mine, step)], 1, 0).astype(BF16)
        other[:, c : c + step] = mm(inner, wd[:, pl.ds(theirs, step)], 1, 0).astype(BF16)


def pair_sum_kernel(own, both, out):
    tp = lax.axis_index("tp")
    out[...] = (own[...].astype(F32) + both[1 - tp].astype(F32)).astype(BF16)


def ffn_sum_kernel(x, hidden, out):
    per = x.shape[1]
    tp = lax.axis_index("tp")
    total = hidden[pl.ds(pl.multiple_of(tp * per, per), per), :]
    for d in range(x.shape[0]):
        total += x[d].astype(F32)
    out[...] = total


def total_of(x):
    return jnp.sum(jnp.sum(x, 0, keepdims=True), 1, keepdims=True)


def final_norm_kernel(x, gain, out):
    p = x[...]
    count = p.shape[0] * p.shape[1]
    mean = total_of(p) / count
    var = total_of(p * p) / count - mean * mean
    normed = ((p - mean) * lax.rsqrt(var + 1e-05) * gain[...]).astype(BF16)
    lines = p.shape[0]
    d = lax.broadcasted_iota(jnp.int32, (SEQS, lines), 0)
    line = lax.broadcasted_iota(jnp.int32, (SEQS, lines), 1)
    spread = (d * lines // SEQS == line).astype(F32).astype(BF16)
    out[...] = mm(spread, normed, 1, 0)


def place_kernel(x, out):
    cols = out.shape[0]
    offset = (lax.axis_index("kv_1") % 2) * (2 * cols) + lax.axis_index("tp") * cols
    col = lax.broadcasted_iota(jnp.int32, (cols, LANES), 0)
    lane = lax.broadcasted_iota(jnp.int32, (cols, LANES), 1)
    pick = (lane == col + offset).astype(F32).astype(BF16)
    out[...] = mm(pick, x[...].astype(BF16), 1, 1).astype(BF16)


def on_device(
    tokens,
    positions,
    state,
    w_query,
    w_key,
    w_value,
    w_gate,
    w_out,
    gain_mix,
    w_ffn_gate,
    w_ffn_up,
    w_ffn_down,
    gain_out,
):
    heads, dim = state.shape[1], state.shape[2]
    width = w_ffn_gate.shape[0]
    cols = w_out.shape[1]
    proj = 4 * heads
    half = width // 2
    tp = lax.axis_index("tp")

    inverse = 10000.0 ** (-jnp.arange(dim // 2, dtype=F32) / (dim // 2))
    angle = positions.astype(F32)[:, None] * inverse[None, :]
    cosine = jnp.cos(angle)
    sine = jnp.sin(angle)
    head_ids = (tp * heads + jnp.arange(heads, dtype=jnp.int32)).astype(F32)
    decay = 1.0 - 2.0 ** (-5.0 - 6.0 * head_ids / (2 * heads - 1))
    aux = jnp.concatenate(
        [
            jnp.concatenate([cosine, cosine], 1),
            jnp.concatenate([-sine, sine], 1),
            jnp.zeros((6, dim), F32),
            jnp.broadcast_to(decay[:, None], (heads, dim)),
        ],
        0,
    )

    tokens_in, aux = lax.optimization_barrier((tokens, aux))
    depth = w_out.shape[0]
    parts = pl.pallas_call(
        project_kernel,
        out_shape=sds((NY, NZ, proj * dim + depth * cols // NZ + LANES), BF16),
        in_specs=[pl.BlockSpec(memory_space=pl.ANY)] * 6,
        out_specs=pl.BlockSpec(memory_space=pl.ANY),
        scratch_shapes=[
            pltpu.VMEM(tokens.shape, BF16),
            pltpu.VMEM((4, *w_query.shape), BF16),
            pltpu.VMEM((4, NY, NZ, w_query.shape[1]), BF16),
            pltpu.VMEM((NY, NZ, LANES), BF16),
            pltpu.SemaphoreType.DMA((5,)),
            pltpu.SemaphoreType.DMA((5,)),
            pltpu.SemaphoreType.DMA((cols // NZ, NY)),
        ],
        interpret=INTERPRET,
        name="project",
    )(tokens_in, w_query, w_key, w_value, w_gate, w_out.T)
    shared = lax.all_to_all(parts, "kv_1", 0, 0, tiled=True)
    near = kernel_call(
        near_sum_kernel,
        sds((NZ, proj, dim), BF16),
        1,
        scratch=[pltpu.VMEM((NZ, proj, dim), F32)],
        name="near_sum",
    )(shared)
    far = lax.all_to_all(near, "kv_0", 0, 0, tiled=True)
    new_state, attended = pl.pallas_call(
        retention_kernel,
        out_shape=[sds(state.shape, F32), sds((NZ, heads, dim), BF16)],
        in_specs=[VMEM] * 3,
        out_specs=[pl.BlockSpec(memory_space=pl.ANY), VMEM],
        scratch_shapes=[pltpu.VMEM(state.shape[1:], F32), pltpu.SemaphoreType.DMA((heads,))],
        compiler_params=PARAMS,
        interpret=INTERPRET,
        name="retention",
    )(far, aux, state)
    gathered = lax.all_to_all(attended, "kv_0", 0, 0, tiled=True)
    gathered = lax.all_gather(gathered, "tp", axis=0)
    mixed = kernel_call(
        mix_kernel,
        sds((NZ, NZ, LANES), BF16),
        2,
        scratch=[pltpu.VMEM((2, NZ, heads, dim), F32)],
        name="mix",
    )(gathered, shared)
    rows = lax.all_to_all(mixed, "kv_0", 0, 0, tiled=True)
    rows = jnp.broadcast_to(rows[None], (NY, *rows.shape))
    rows = lax.all_to_all(rows, "kv_1", 0, 0, tiled=True)
    rows = lax.all_gather(rows, "tp", axis=0)
    lines = half // LANES
    own, other, hidden_row = kernel_call(
        feed_kernel,
        [sds((SEQS, half), BF16)] * 2 + [sds((1, width), F32)],
        5,
        scratch=[
            pltpu.VMEM((SEQS, width), F32),
            pltpu.VMEM((SEQS, width), BF16),
            pltpu.VMEM((2, SEQS, LANES), F32),
        ],
        name="feed",
    )(rows, gain_mix[None, :], w_ffn_gate.T, w_ffn_up.T, w_ffn_down)
    both = lax.all_gather(other, "tp", axis=0)
    part = kernel_call(pair_sum_kernel, sds(own.shape, BF16), 2, name="pair_sum")(own, both)
    part = lax.all_to_all(part.reshape(NY, NZ, half), "kv_1", 0, 0, tiled=True)
    part = kernel_call(
        near_sum_kernel,
        sds((NZ, lines, LANES), BF16),
        1,
        scratch=[pltpu.VMEM((NZ, lines, LANES), F32)],
        name="half_sum",
    )(part)
    part = lax.all_to_all(part, "kv_0", 0, 0, tiled=True)
    summed = kernel_call(ffn_sum_kernel, sds((lines, LANES), F32), 2, name="ffn_sum")(
        part, hidden_row.reshape(2 * lines, LANES)
    )
    summed = lax.all_gather(summed, "tp", axis=0, tiled=True)
    spread = kernel_call(final_norm_kernel, sds((SEQS, LANES), F32), 2, name="final_norm")(
        summed, gain_out.reshape(2 * lines, LANES)
    )
    spread = lax.all_to_all(spread.reshape(SEQS, 1, LANES), KV, 0, 0, tiled=True)
    layer_out = kernel_call(place_kernel, sds((cols, SEQS), BF16), 1, name="place")(
        spread.reshape(SEQS, LANES)
    )
    return (layer_out.T, new_state)


def solution(mesh):
    finer = Mesh(
        mesh.devices.reshape(mesh.shape["dp"], NZ, NY, mesh.shape["tp"]),
        ("dp", "kv_0", "kv_1", "tp"),
    )
    return jax.shard_map(
        on_device,
        mesh=finer,
        in_specs=(
            P("dp", KV),
            P(DP_KV),
            P(DP_KV, "tp", None, None),
            P(KV, "tp"),
            P(KV, "tp"),
            P(KV, "tp"),
            P(KV, "tp"),
            P(None, KV_TP),
            P(),
            P(None, KV_TP),
            P(None, KV_TP),
            P(KV_TP, None),
            P(),
        ),
        out_specs=(P("dp", KV_TP), P(DP_KV, "tp", None, None)),
        check_vma=False,
    )
```

```python
import jax
import jax.numpy as jnp
from jax import lax
from jax.experimental import pallas as pl
from jax.experimental.pallas import tpu as pltpu
from jax.sharding import Mesh
from jax.sharding import PartitionSpec as P

KV = ("kv_0", "kv_1")
KV_TP = ("kv_0", "kv_1", "tp")
DP_KV = ("dp", "kv_0", "kv_1")
F32 = jnp.float32
BF16 = jnp.bfloat16
LANES = 128
NZ = 16
NY = 4
SEQS = NZ * NY
ORDER_0 = (0, 3, 1, 2)
ORDER_1 = (2, 0, 3, 1)
INTERPRET = False

VMEM = pl.BlockSpec(memory_space=pltpu.VMEM)
PARAMS = pltpu.CompilerParams(vmem_limit_bytes=32 * 1024 * 1024)


def kernel_call(body, out_shape, n_in, scratch=(), name=None):
    single = not isinstance(out_shape, (list, tuple))
    return pl.pallas_call(
        body,
        out_shape=out_shape,
        in_specs=[VMEM] * n_in,
        out_specs=VMEM if single else [VMEM] * len(out_shape),
        scratch_shapes=list(scratch),
        compiler_params=PARAMS,
        interpret=INTERPRET,
        name=name,
    )


def sds(shape, dtype):
    return jax.ShapeDtypeStruct(shape, dtype)


def rows_of(s):
    return (s % NY) * NZ + s // NY


def perm_matrix(dtype):
    d = lax.broadcasted_iota(jnp.int32, (SEQS, SEQS), 0)
    s = lax.broadcasted_iota(jnp.int32, (SEQS, SEQS), 1)
    return (d == rows_of(s)).astype(F32).astype(dtype)


def mm(a, b, ca, cb):
    return lax.dot_general(a, b, (((ca,), (cb,)), ((), ())), preferred_element_type=F32)


def project_kernel(
    tok_hbm, wq, wk, wv, wg, w_out, out_hbm,
    tok, weights, out, share, residual, sems, out_sems, share_sems,
):
    sources = (wq, wk, wv, wg)
    count = len(sources)
    width = weights.shape[2]
    copies = [pltpu.make_async_copy(tok_hbm, tok, sems.at[count])]
    for i, w in enumerate(sources):
        copies.append(pltpu.make_async_copy(w, weights.at[i], sems.at[i]))
    for copy in copies:
        copy.start()
    load = pltpu.make_async_copy(w_out, share, sems.at[count + 1])
    load.start()
    sends = []
    copies[0].wait()
    rows = mm(perm_matrix(BF16), tok[...], 1, 0).astype(BF16)
    residual[...] = jnp.zeros(residual.shape, BF16)
    for y in range(NY):
        residual[y, :, 0 : rows.shape[1]] = rows[y * NZ : (y + 1) * NZ]
    tail = pl.ds(out_hbm.shape[2] - LANES, LANES)
    sends.append(pltpu.make_async_copy(residual, out_hbm.at[:, :, tail], out_sems.at[count]))
    sends[-1].start()
    for i in range(count):
        copies[1 + i].wait()
        out[i] = mm(rows, weights[i], 1, 0).astype(BF16).reshape(NY, NZ, width)
        cols = pl.ds(i * width, width)
        sends.append(pltpu.make_async_copy(out.at[i], out_hbm.at[:, :, cols], out_sems.at[i]))
        sends[-1].start()
    load.wait()
    depth = share.shape[1]
    for part in range(share.shape[0] // NZ):
        cols = pl.ds(count * width + part * depth, depth)
        for y in range(NY):
            sends.append(
                pltpu.make_async_copy(
                    share.at[pl.ds(part * NZ, NZ)], out_hbm.at[y, :, cols], share_sems.at[part, y]
                )
            )
            sends[-1].start()
    for send in sends:
        send.wait()


def near_sum_kernel(x, out, wide):
    for c in range(wide.shape[1]):
        cols = slice(c * LANES, (c + 1) * LANES)
        total = x[0, :, cols].astype(F32)
        for y in range(1, NY):
            total += x[y, :, cols].astype(F32)
        wide[:, c, :] = total
    out[...] = wide[...].astype(BF16)


def retention_kernel(x, aux, state, state_out, out, new_state, sems):
    heads, dim = state.shape[1], state.shape[2]
    total = x[0].astype(F32)
    for z in range(1, NZ):
        total += x[z].astype(F32)
    cosine = aux[0:1, :]
    sine = aux[1:2, :]
    query = total[0:heads]
    key = total[heads : 2 * heads]
    value = total[2 * heads : 3 * heads]
    gate = total[3 * heads : 4 * heads]
    query = query * cosine + pltpu.roll(query, dim // 2, 1) * sine
    key = (key * cosine + pltpu.roll(key, dim // 2, 1) * sine) * dim ** (-0.5)
    query_t = query.T
    key_t = key.T
    lines = []
    sends = []
    for h in range(heads):
        updated = aux[8 + h : 9 + h, :] * state[0, h] + key_t[:, h : h + 1] * value[h : h + 1, :]
        new_state[h] = updated
        sends.append(pltpu.make_async_copy(new_state.at[h], state_out.at[0, h], sems.at[h]))
        sends[h].start()
        lines.append(jnp.sum(query_t[:, h : h + 1] * updated, axis=0, keepdims=True))
    retained = jnp.concatenate(lines, axis=0)
    mean = jnp.mean(retained, -1, keepdims=True)
    var = jnp.mean(jnp.square(retained - mean), -1, keepdims=True)
    normed = (retained - mean) * lax.rsqrt(var + 1e-05)
    silu = gate / (1.0 + jnp.exp(-gate))
    attended = (normed * silu).astype(BF16)
    out[...] = jnp.broadcast_to(attended[None], out.shape)
    for send in sends:
        send.wait()


def mix_kernel(x, shared, out, wide):
    tp = lax.axis_index("tp")
    tps, _, heads, dim = x.shape
    cols = LANES // NY
    depth = tps * heads * dim
    first = shared.shape[2] - LANES - 2 * depth
    wide[...] = x[...].astype(F32)
    owners = [jnp.where(tp == 0, even, odd) for even, odd in zip(ORDER_0, ORDER_1)]
    own = lax.broadcasted_iota(jnp.int32, (LANES, LANES), 0)
    lane = lax.broadcasted_iota(jnp.int32, (LANES, LANES), 1)
    acc = jnp.zeros((NZ, LANES), F32)
    for b, y in enumerate(owners):
        pick = (own == tp * cols + lane % cols) & (lane // cols == b)
        pick = pick.astype(F32).astype(BF16)
        acc += mm(shared[y, :, first + 2 * depth :], pick, 1, 0)
    for t in range(tps):
        for h in range(heads):
            k = first + (t * heads + h) * dim
            pieces = []
            for y in owners:
                pieces.append(shared[y, :, k : k + dim])
                pieces.append(shared[y, :, k + depth : k + depth + dim])
            weight = jnp.concatenate(pieces, axis=0)
            acc += mm(wide[t, :, h, :].astype(BF16), weight, 1, 1)
    out[...] = jnp.broadcast_to(acc.astype(BF16)[None], out.shape)


def feed_kernel(x, gain, wg_t, wu_t, wd, own, other, row, wide, narrow, stats):
    per = x.shape[3]
    tp = lax.axis_index("tp")
    place = lax.axis_index("kv_1") * NZ + lax.axis_index("kv_0")
    cols = LANES // NY
    width = wide.shape[1]
    odd = (lax.broadcasted_iota(jnp.int32, (per, LANES), 1) // cols) % 2 == 1
    sums = [jnp.zeros((per, LANES), F32) for _ in range(NY)]
    squares = [jnp.zeros((per, LANES), F32) for _ in range(NY)]
    for z in range(NZ):
        for y in range(NY):
            a = x[0, y, z].astype(F32)
            b = x[1, y, z].astype(F32)
            low = jnp.where(odd, b, a)
            high = pltpu.roll(jnp.where(odd, a, b), cols, 1)
            wide[y * per : (y + 1) * per, 2 * z * LANES : (2 * z + 1) * LANES] = low
            wide[y * per : (y + 1) * per, (2 * z + 1) * LANES : (2 * z + 2) * LANES] = high
            sums[y] += low + high
            squares[y] += low * low + high * high
    mean = jnp.sum(jnp.concatenate(sums, 0), -1, keepdims=True) / width
    var = jnp.sum(jnp.concatenate(squares, 0), -1, keepdims=True) / width - mean * mean
    scale = lax.rsqrt(var + 1e-05)
    stats[0] = jnp.broadcast_to(mean, stats.shape[1:])
    stats[1] = jnp.broadcast_to(scale, stats.shape[1:])
    for a in range(width // LANES):
        c = slice(a * LANES, (a + 1) * LANES)
        narrow[:, c] = ((wide[:, c] - mean) * scale * gain[:, c]).astype(BF16)
    own_mean = stats[0, pl.ds(place, 1), 0:1]
    own_scale = stats[1, pl.ds(place, 1), 0:1]
    own_row = (wide[pl.ds(place, 1), :] - own_mean) * own_scale * gain[...]
    row[...] = own_row.astype(BF16).astype(F32)
    gate = mm(narrow[...], wg_t[...], 1, 1)
    up = mm(narrow[...], wu_t[...], 1, 1)
    inner = (gate / (1.0 + jnp.exp(-gate)) * up).astype(BF16)
    half = own.shape[1]
    step = 4 * LANES
    for c in range(0, half, step):
        mine = pl.multiple_of(tp * half + c, step)
        theirs = pl.multiple_of((1 - tp) * half + c, step)
        own[:, c : c + step] = mm(inner, wd[:, pl.ds(mine, step)], 1, 0).astype(BF16)
        other[:, c : c + step] = mm(inner, wd[:, pl.ds(theirs, step)], 1, 0).astype(BF16)


def pair_sum_kernel(own, both, out):
    tp = lax.axis_index("tp")
    out[...] = (own[...].astype(F32) + both[1 - tp].astype(F32)).astype(BF16)


def ffn_sum_kernel(x, hidden, out):
    per = x.shape[1]
    tp = lax.axis_index("tp")
    total = hidden[pl.ds(pl.multiple_of(tp * per, per), per), :]
    for d in range(x.shape[0]):
        total += x[d].astype(F32)
    out[...] = total


def total_of(x):
    return jnp.sum(jnp.sum(x, 0, keepdims=True), 1, keepdims=True)


def final_norm_kernel(x, gain, out):
    p = x[...]
    count = p.shape[0] * p.shape[1]
    mean = total_of(p) / count
    var = total_of(p * p) / count - mean * mean
    normed = ((p - mean) * lax.rsqrt(var + 1e-05) * gain[...]).astype(BF16)
    lines = p.shape[0]
    d = lax.broadcasted_iota(jnp.int32, (SEQS, lines), 0)
    line = lax.broadcasted_iota(jnp.int32, (SEQS, lines), 1)
    spread = (d * lines // SEQS == line).astype(F32).astype(BF16)
    out[...] = mm(spread, normed, 1, 0)


def place_kernel(x, out):
    cols = out.shape[0]
    offset = (lax.axis_index("kv_1") % 2) * (2 * cols) + lax.axis_index("tp") * cols
    col = lax.broadcasted_iota(jnp.int32, (cols, LANES), 0)
    lane = lax.broadcasted_iota(jnp.int32, (cols, LANES), 1)
    pick = (lane == col + offset).astype(F32).astype(BF16)
    out[...] = mm(pick, x[...].astype(BF16), 1, 1).astype(BF16)


def on_device(
    tokens,
    positions,
    state,
    w_query,
    w_key,
    w_value,
    w_gate,
    w_out,
    gain_mix,
    w_ffn_gate,
    w_ffn_up,
    w_ffn_down,
    gain_out,
):
    heads, dim = state.shape[1], state.shape[2]
    width = w_ffn_gate.shape[0]
    cols = w_out.shape[1]
    proj = 4 * heads
    half = width // 2
    tp = lax.axis_index("tp")

    inverse = 10000.0 ** (-jnp.arange(dim // 2, dtype=F32) / (dim // 2))
    angle = positions.astype(F32)[:, None] * inverse[None, :]
    cosine = jnp.cos(angle)
    sine = jnp.sin(angle)
    head_ids = (tp * heads + jnp.arange(heads, dtype=jnp.int32)).astype(F32)
    decay = 1.0 - 2.0 ** (-5.0 - 6.0 * head_ids / (2 * heads - 1))
    aux = jnp.concatenate(
        [
            jnp.concatenate([cosine, cosine], 1),
            jnp.concatenate([-sine, sine], 1),
            jnp.zeros((6, dim), F32),
            jnp.broadcast_to(decay[:, None], (heads, dim)),
        ],
        0,
    )

    tokens_in, aux = lax.optimization_barrier((tokens, aux))
    depth = w_out.shape[0]
    parts = pl.pallas_call(
        project_kernel,
        out_shape=sds((NY, NZ, proj * dim + depth * cols // NZ + LANES), BF16),
        in_specs=[pl.BlockSpec(memory_space=pl.ANY)] * 6,
        out_specs=pl.BlockSpec(memory_space=pl.ANY),
        scratch_shapes=[
            pltpu.VMEM(tokens.shape, BF16),
            pltpu.VMEM((4, *w_query.shape), BF16),
            pltpu.VMEM((4, NY, NZ, w_query.shape[1]), BF16),
            pltpu.VMEM((cols, depth), BF16),
            pltpu.VMEM((NY, NZ, LANES), BF16),
            pltpu.SemaphoreType.DMA((6,)),
            pltpu.SemaphoreType.DMA((5,)),
            pltpu.SemaphoreType.DMA((cols // NZ, NY)),
        ],
        interpret=INTERPRET,
        name="project",
    )(tokens_in, w_query, w_key, w_value, w_gate, w_out.T)
    shared = lax.all_to_all(parts, "kv_1", 0, 0, tiled=True)
    near = kernel_call(
        near_sum_kernel,
        sds((NZ, proj, dim), BF16),
        1,
        scratch=[pltpu.VMEM((NZ, proj, dim), F32)],
        name="near_sum",
    )(shared)
    far = lax.all_to_all(near, "kv_0", 0, 0, tiled=True)
    new_state, attended = pl.pallas_call(
        retention_kernel,
        out_shape=[sds(state.shape, F32), sds((NZ, heads, dim), BF16)],
        in_specs=[VMEM] * 3,
        out_specs=[pl.BlockSpec(memory_space=pl.ANY), VMEM],
        scratch_shapes=[pltpu.VMEM(state.shape[1:], F32), pltpu.SemaphoreType.DMA((heads,))],
        compiler_params=PARAMS,
        interpret=INTERPRET,
        name="retention",
    )(far, aux, state)
    gathered = lax.all_to_all(attended, "kv_0", 0, 0, tiled=True)
    gathered = lax.all_gather(gathered, "tp", axis=0)
    mixed = kernel_call(
        mix_kernel,
        sds((NZ, NZ, LANES), BF16),
        2,
        scratch=[pltpu.VMEM((2, NZ, heads, dim), F32)],
        name="mix",
    )(gathered, shared)
    rows = lax.all_to_all(mixed, "kv_0", 0, 0, tiled=True)
    rows = jnp.broadcast_to(rows[None], (NY, *rows.shape))
    rows = lax.all_to_all(rows, "kv_1", 0, 0, tiled=True)
    rows = lax.all_gather(rows, "tp", axis=0)
    lines = half // LANES
    own, other, hidden_row = kernel_call(
        feed_kernel,
        [sds((SEQS, half), BF16)] * 2 + [sds((1, width), F32)],
        5,
        scratch=[
            pltpu.VMEM((SEQS, width), F32),
            pltpu.VMEM((SEQS, width), BF16),
            pltpu.VMEM((2, SEQS, LANES), F32),
        ],
        name="feed",
    )(rows, gain_mix[None, :], w_ffn_gate.T, w_ffn_up.T, w_ffn_down)
    both = lax.all_gather(other, "tp", axis=0)
    part = kernel_call(pair_sum_kernel, sds(own.shape, BF16), 2, name="pair_sum")(own, both)
    part = lax.all_to_all(part.reshape(NY, NZ, half), "kv_1", 0, 0, tiled=True)
    part = kernel_call(
        near_sum_kernel,
        sds((NZ, lines, LANES), BF16),
        1,
        scratch=[pltpu.VMEM((NZ, lines, LANES), F32)],
        name="half_sum",
    )(part)
    part = lax.all_to_all(part, "kv_0", 0, 0, tiled=True)
    summed = kernel_call(ffn_sum_kernel, sds((lines, LANES), F32), 2, name="ffn_sum")(
        part, hidden_row.reshape(2 * lines, LANES)
    )
    summed = lax.all_gather(summed, "tp", axis=0, tiled=True)
    spread = kernel_call(final_norm_kernel, sds((SEQS, LANES), F32), 2, name="final_norm")(
        summed, gain_out.reshape(2 * lines, LANES)
    )
    spread = lax.all_to_all(spread.reshape(SEQS, 1, LANES), KV, 0, 0, tiled=True)
    layer_out = kernel_call(place_kernel, sds((cols, SEQS), BF16), 1, name="place")(
        spread.reshape(SEQS, LANES)
    )
    return (layer_out.T, new_state)


def solution(mesh):
    finer = Mesh(
        mesh.devices.reshape(mesh.shape["dp"], NZ, NY, mesh.shape["tp"]),
        ("dp", "kv_0", "kv_1", "tp"),
    )
    return jax.shard_map(
        on_device,
        mesh=finer,
        in_specs=(
            P("dp", KV),
            P(DP_KV),
            P(DP_KV, "tp", None, None),
            P(KV, "tp"),
            P(KV, "tp"),
            P(KV, "tp"),
            P(KV, "tp"),
            P(None, KV_TP),
            P(),
            P(None, KV_TP),
            P(None, KV_TP),
            P(KV_TP, None),
            P(),
        ),
        out_specs=(P("dp", KV_TP), P(DP_KV, "tp", None, None)),
        check_vma=False,
    )
```

```python
import jax
import jax.numpy as jnp
from jax import lax
from jax.experimental import pallas as pl
from jax.experimental.pallas import tpu as pltpu
from jax.sharding import Mesh
from jax.sharding import PartitionSpec as P

KV = ("kv_0", "kv_1")
YZ = ("kv_1", "kv_0")
Z_TP = ("kv_0", "tp")
Y_TP = ("kv_1", "tp")
KV_TP = ("kv_0", "kv_1", "tp")
DP_KV = ("dp", "kv_0", "kv_1")
F32 = jnp.float32
BF16 = jnp.bfloat16
LANES = 128
NZ = 16
NY = 4
SEQS = NZ * NY
INTERPRET = False

VMEM = pl.BlockSpec(memory_space=pltpu.VMEM)
PARAMS = pltpu.CompilerParams(vmem_limit_bytes=32 * 1024 * 1024)


def kernel_call(body, out_shape, n_in, scratch=(), name=None):
    single = not isinstance(out_shape, (list, tuple))
    return pl.pallas_call(
        body,
        out_shape=out_shape,
        in_specs=[VMEM] * n_in,
        out_specs=VMEM if single else [VMEM] * len(out_shape),
        scratch_shapes=list(scratch),
        compiler_params=PARAMS,
        interpret=INTERPRET,
        name=name,
    )


def sds(shape, dtype):
    return jax.ShapeDtypeStruct(shape, dtype)


def far_z(z):
    return z // (NZ // 2)


def far_y(y):
    return y // (NY // 2)


Z_GROUPS = [[z * 2 + (t ^ far_z(z)) for z in range(NZ)] for t in range(2)]
Y_GROUPS = [[y * 2 + (t ^ far_y(y)) for y in range(NY)] for t in range(2)]
ALL_GROUPS = [
    [(z * NY + y) * 2 + (t ^ far_z(z)) for z in range(NZ) for y in range(NY)] for t in range(2)
]


def exchange(x, axes, groups):
    return lax.all_to_all(x, axes, 0, 0, tiled=True, axis_index_groups=groups)


def own_side():
    return (far_z(lax.axis_index("kv_0")) + far_y(lax.axis_index("kv_1"))) % 2


def own_half():
    return (lax.axis_index("tp") + own_side()) % 2


def rows_of(s):
    return (s % NY) * NZ + s // NY


def perm_matrix(dtype):
    d = lax.broadcasted_iota(jnp.int32, (SEQS, SEQS), 0)
    s = lax.broadcasted_iota(jnp.int32, (SEQS, SEQS), 1)
    return (d == rows_of(s)).astype(F32).astype(dtype)


def mm(a, b, ca, cb):
    return lax.dot_general(a, b, (((ca,), (cb,)), ((), ())), preferred_element_type=F32)


def project_kernel(tok_hbm, wq, wk, wv, wg, out_hbm, tok, weights, out, sems, out_sems):
    sources = (wq, wk, wv, wg)
    count = len(sources)
    width = weights.shape[2]
    copies = [pltpu.make_async_copy(tok_hbm, tok, sems.at[count])]
    for i, w in enumerate(sources):
        copies.append(pltpu.make_async_copy(w, weights.at[i], sems.at[i]))
    for copy in copies:
        copy.start()
    copies[0].wait()
    rows = mm(perm_matrix(BF16), tok[...], 1, 0).astype(BF16)
    sends = []
    for i in range(count):
        copies[1 + i].wait()
        out[i] = mm(rows, weights[i], 1, 0).astype(BF16).reshape(NY, NZ, width)
        cols = pl.ds(i * width, width)
        sends.append(pltpu.make_async_copy(out.at[i], out_hbm.at[:, :, cols], out_sems.at[i]))
        sends[i].start()
    for send in sends:
        send.wait()


def near_sum_kernel(x, out, wide):
    for c in range(wide.shape[1]):
        cols = slice(c * LANES, (c + 1) * LANES)
        total = x[0, :, cols].astype(F32)
        for y in range(1, NY):
            total += x[y, :, cols].astype(F32)
        wide[:, c, :] = total
    out[...] = wide[...].astype(BF16)


def retention_kernel(x, aux, state, state_out, out, new_state, sems):
    heads, dim = state.shape[1], state.shape[2]
    total = x[0].astype(F32)
    for z in range(1, NZ):
        total += x[z].astype(F32)
    cosine = aux[0:1, :]
    sine = aux[1:2, :]
    query = total[0:heads]
    key = total[heads : 2 * heads]
    value = total[2 * heads : 3 * heads]
    gate = total[3 * heads : 4 * heads]
    query = query * cosine + pltpu.roll(query, dim // 2, 1) * sine
    key = (key * cosine + pltpu.roll(key, dim // 2, 1) * sine) * dim ** (-0.5)
    query_t = query.T
    key_t = key.T
    lines = []
    sends = []
    for h in range(heads):
        updated = aux[8 + h : 9 + h, :] * state[0, h] + key_t[:, h : h + 1] * value[h : h + 1, :]
        new_state[h] = updated
        sends.append(pltpu.make_async_copy(new_state.at[h], state_out.at[0, h], sems.at[h]))
        sends[h].start()
        lines.append(jnp.sum(query_t[:, h : h + 1] * updated, axis=0, keepdims=True))
    retained = jnp.concatenate(lines, axis=0)
    mean = jnp.mean(retained, -1, keepdims=True)
    var = jnp.mean(jnp.square(retained - mean), -1, keepdims=True)
    normed = (retained - mean) * lax.rsqrt(var + 1e-05)
    silu = gate / (1.0 + jnp.exp(-gate))
    attended = (normed * silu).astype(BF16)
    out[...] = jnp.broadcast_to(attended[None], out.shape)
    for send in sends:
        send.wait()


def mix_kernel(x, w_t, tok, out, wide):
    tp = lax.axis_index("tp")
    tps, seqs, heads, dim = x.shape
    cols = w_t.shape[0]
    groups = LANES // cols
    wide[...] = x[...].astype(F32)
    own = lax.broadcasted_iota(jnp.int32, (tok.shape[1], LANES), 0)
    lane = lax.broadcasted_iota(jnp.int32, (tok.shape[1], LANES), 1)
    pick = (own == tp * cols + lane % cols).astype(F32).astype(BF16)
    rows = mm(perm_matrix(BF16), tok[...], 1, 0).astype(BF16)
    acc = mm(rows, pick, 1, 0)
    w4 = jnp.concatenate([w_t[...]] * groups, axis=0)
    for t in range(tps):
        for h in range(heads):
            k = (t * heads + h) * dim
            acc += mm(wide[t, :, h, :].astype(BF16), w4[:, k : k + dim], 1, 1)
    per = seqs // groups
    turn = (lax.axis_index("kv_1") % (groups // tps)) * tps + tp
    block = lax.broadcasted_iota(jnp.int32, (per, LANES), 1) // cols
    block = (block + groups - turn) % groups
    packed = acc[0:per]
    for g in range(1, groups):
        packed = jnp.where(block == g, acc[g * per : (g + 1) * per], packed)
    out[...] = jnp.broadcast_to(packed.astype(BF16)[None], out.shape)


def feed_kernel(x, gain, wg_t, wu_t, wd, own, other, row, wide, narrow, stats):
    tps = x.shape[0]
    per = x.shape[3]
    side = own_side()
    cores = (side, 1 - side)
    tp = own_half()
    place = lax.axis_index("kv_1") * NZ + lax.axis_index("kv_0")
    groups = SEQS // per
    cols = LANES // groups
    chips = groups // tps
    width = wide.shape[1]
    lane = lax.broadcasted_iota(jnp.int32, (per, LANES), 1) // cols
    sums = [jnp.zeros((per, LANES), F32) for _ in range(groups)]
    squares = [jnp.zeros((per, LANES), F32) for _ in range(groups)]
    for a in range(SEQS // chips):
        sources = []
        for q in range(groups):
            kv = a * chips + q // tps
            y, z = kv % NY, kv // NY
            core = cores[(q % tps) ^ far_y(y) ^ far_z(z)]
            sources.append(x[core, y, z].astype(F32))
        for g in range(groups):
            tile = sources[(groups - g) % groups]
            for j in range(1, groups):
                tile = jnp.where(lane == j, sources[(j - g) % groups], tile)
            if g:
                tile = pltpu.roll(tile, LANES - g * cols, 1)
            wide[g * per : (g + 1) * per, a * LANES : (a + 1) * LANES] = tile
            sums[g] += tile
            squares[g] += tile * tile
    mean = jnp.sum(jnp.concatenate(sums, 0), -1, keepdims=True) / width
    var = jnp.sum(jnp.concatenate(squares, 0), -1, keepdims=True) / width - mean * mean
    scale = lax.rsqrt(var + 1e-05)
    stats[0] = jnp.broadcast_to(mean, stats.shape[1:])
    stats[1] = jnp.broadcast_to(scale, stats.shape[1:])
    for a in range(width // LANES):
        c = slice(a * LANES, (a + 1) * LANES)
        narrow[:, c] = ((wide[:, c] - mean) * scale * gain[:, c]).astype(BF16)
    own_mean = stats[0, pl.ds(place, 1), 0:1]
    own_scale = stats[1, pl.ds(place, 1), 0:1]
    own_row = (wide[pl.ds(place, 1), :] - own_mean) * own_scale * gain[...]
    row[...] = own_row.astype(BF16).astype(F32)
    gate = mm(narrow[...], wg_t[...], 1, 1)
    up = mm(narrow[...], wu_t[...], 1, 1)
    inner = (gate / (1.0 + jnp.exp(-gate)) * up).astype(BF16)
    half = own.shape[1]
    step = 4 * LANES
    for c in range(0, half, step):
        mine = pl.multiple_of(tp * half + c, step)
        theirs = pl.multiple_of((1 - tp) * half + c, step)
        own[:, c : c + step] = mm(inner, wd[:, pl.ds(mine, step)], 1, 0).astype(BF16)
        other[:, c : c + step] = mm(inner, wd[:, pl.ds(theirs, step)], 1, 0).astype(BF16)


def pair_sum_kernel(own, both, out):
    tp = lax.axis_index("tp")
    out[...] = (own[...].astype(F32) + both[1 - tp].astype(F32)).astype(BF16)


def ffn_sum_kernel(x, hidden, out):
    per = x.shape[1]
    total = hidden[pl.ds(pl.multiple_of(own_half() * per, per), per), :]
    for d in range(x.shape[0]):
        total += x[d].astype(F32)
    out[...] = total


def total_of(x):
    return jnp.sum(jnp.sum(x, 0, keepdims=True), 1, keepdims=True)


def final_norm_kernel(x, gain, out):
    side = own_side()
    p = jnp.concatenate([x[side], x[1 - side]], axis=0)
    count = p.shape[0] * p.shape[1]
    mean = total_of(p) / count
    var = total_of(p * p) / count - mean * mean
    normed = ((p - mean) * lax.rsqrt(var + 1e-05) * gain[...]).astype(BF16)
    lines = p.shape[0]
    d = lax.broadcasted_iota(jnp.int32, (SEQS, lines), 0)
    line = lax.broadcasted_iota(jnp.int32, (SEQS, lines), 1)
    spread = (d * lines // SEQS == line).astype(F32).astype(BF16)
    out[...] = mm(spread, normed, 1, 0)


def place_kernel(x, out):
    cols = out.shape[0]
    offset = (lax.axis_index("kv_1") % 2) * (2 * cols) + lax.axis_index("tp") * cols
    col = lax.broadcasted_iota(jnp.int32, (cols, LANES), 0)
    lane = lax.broadcasted_iota(jnp.int32, (cols, LANES), 1)
    pick = (lane == col + offset).astype(F32).astype(BF16)
    out[...] = mm(pick, x[...].astype(BF16), 1, 1).astype(BF16)


def on_device(
    tokens,
    positions,
    state,
    w_query,
    w_key,
    w_value,
    w_gate,
    w_out,
    gain_mix,
    w_ffn_gate,
    w_ffn_up,
    w_ffn_down,
    gain_out,
):
    heads, dim = state.shape[1], state.shape[2]
    width = w_ffn_gate.shape[0]
    cols = w_out.shape[1]
    proj = 4 * heads
    half = width // 2
    tp = lax.axis_index("tp")

    inverse = 10000.0 ** (-jnp.arange(dim // 2, dtype=F32) / (dim // 2))
    angle = positions.astype(F32)[:, None] * inverse[None, :]
    cosine = jnp.cos(angle)
    sine = jnp.sin(angle)
    head_ids = (tp * heads + jnp.arange(heads, dtype=jnp.int32)).astype(F32)
    decay = 1.0 - 2.0 ** (-5.0 - 6.0 * head_ids / (2 * heads - 1))
    aux = jnp.concatenate(
        [
            jnp.concatenate([cosine, cosine], 1),
            jnp.concatenate([-sine, sine], 1),
            jnp.zeros((6, dim), F32),
            jnp.broadcast_to(decay[:, None], (heads, dim)),
        ],
        0,
    )

    tokens_in, aux = lax.optimization_barrier((tokens, aux))
    parts = pl.pallas_call(
        project_kernel,
        out_shape=sds((NY, NZ, proj * dim), BF16),
        in_specs=[pl.BlockSpec(memory_space=pl.ANY)] * 5,
        out_specs=pl.BlockSpec(memory_space=pl.ANY),
        scratch_shapes=[
            pltpu.VMEM(tokens.shape, BF16),
            pltpu.VMEM((4, *w_query.shape), BF16),
            pltpu.VMEM((4, NY, NZ, w_query.shape[1]), BF16),
            pltpu.SemaphoreType.DMA((5,)),
            pltpu.SemaphoreType.DMA((4,)),
        ],
        interpret=INTERPRET,
        name="project",
    )(tokens_in, w_query, w_key, w_value, w_gate)
    near = lax.all_to_all(parts, "kv_1", 0, 0, tiled=True)
    near = kernel_call(
        near_sum_kernel,
        sds((NZ, proj, dim), BF16),
        1,
        scratch=[pltpu.VMEM((NZ, proj, dim), F32)],
        name="near_sum",
    )(near)
    far = lax.all_to_all(near, "kv_0", 0, 0, tiled=True)
    new_state, attended = pl.pallas_call(
        retention_kernel,
        out_shape=[sds(state.shape, F32), sds((SEQS, heads, dim), BF16)],
        in_specs=[VMEM] * 3,
        out_specs=[pl.BlockSpec(memory_space=pl.ANY), VMEM],
        scratch_shapes=[pltpu.VMEM(state.shape[1:], F32), pltpu.SemaphoreType.DMA((heads,))],
        compiler_params=PARAMS,
        interpret=INTERPRET,
        name="retention",
    )(far, aux, state)
    gathered = lax.all_to_all(attended, YZ, 0, 0, tiled=True)
    gathered = lax.all_gather(gathered, "tp", axis=0)
    per = SEQS * cols // LANES
    mixed = kernel_call(
        mix_kernel,
        sds((NZ, per, LANES), BF16),
        3,
        scratch=[pltpu.VMEM((2, SEQS, heads, dim), F32)],
        name="mix",
    )(gathered.reshape(2, SEQS, heads, dim), w_out.T, tokens)
    rows = exchange(mixed, Z_TP, Z_GROUPS)
    rows = jnp.broadcast_to(rows[None], (NY, *rows.shape))
    rows = exchange(rows, Y_TP, Y_GROUPS)
    rows = lax.all_gather(rows, "tp", axis=0)
    lines = half // LANES
    own, other, hidden_row = kernel_call(
        feed_kernel,
        [sds((SEQS, half), BF16)] * 2 + [sds((1, width), F32)],
        5,
        scratch=[
            pltpu.VMEM((SEQS, width), F32),
            pltpu.VMEM((SEQS, width), BF16),
            pltpu.VMEM((2, SEQS, LANES), F32),
        ],
        name="feed",
    )(rows, gain_mix[None, :], w_ffn_gate.T, w_ffn_up.T, w_ffn_down)
    both = lax.all_gather(other, "tp", axis=0)
    part = kernel_call(pair_sum_kernel, sds(own.shape, BF16), 2, name="pair_sum")(own, both)
    part = exchange(part.reshape(NY, NZ, half), Y_TP, Y_GROUPS)
    part = kernel_call(
        near_sum_kernel,
        sds((NZ, lines, LANES), BF16),
        1,
        scratch=[pltpu.VMEM((NZ, lines, LANES), F32)],
        name="half_sum",
    )(part)
    part = exchange(part, Z_TP, Z_GROUPS)
    summed = kernel_call(ffn_sum_kernel, sds((lines, LANES), F32), 2, name="ffn_sum")(
        part, hidden_row.reshape(2 * lines, LANES)
    )
    summed = lax.all_gather(summed, "tp", axis=0)
    spread = kernel_call(final_norm_kernel, sds((SEQS, LANES), F32), 2, name="final_norm")(
        summed, gain_out.reshape(2 * lines, LANES)
    )
    spread = exchange(spread.reshape(SEQS, 1, LANES), KV_TP, ALL_GROUPS)
    layer_out = kernel_call(place_kernel, sds((cols, SEQS), BF16), 1, name="place")(
        spread.reshape(SEQS, LANES)
    )
    return (layer_out.T, new_state)


def solution(mesh):
    finer = Mesh(
        mesh.devices.reshape(mesh.shape["dp"], NZ, NY, mesh.shape["tp"]),
        ("dp", "kv_0", "kv_1", "tp"),
    )
    return jax.shard_map(
        on_device,
        mesh=finer,
        in_specs=(
            P("dp", KV),
            P(DP_KV),
            P(DP_KV, "tp", None, None),
            P(KV, "tp"),
            P(KV, "tp"),
            P(KV, "tp"),
            P(KV, "tp"),
            P(None, KV_TP),
            P(),
            P(None, KV_TP),
            P(None, KV_TP),
            P(KV_TP, None),
            P(),
        ),
        out_specs=(P("dp", KV_TP), P(DP_KV, "tp", None, None)),
        check_vma=False,
    )
```

```python
import math

import jax
import jax.numpy as jnp
from jax import lax
from jax.experimental import pallas as pl
from jax.experimental.pallas import tpu as pltpu
from jax.sharding import Mesh
from jax.sharding import PartitionSpec as P

KV = ("kv_0", "kv_1")
YZ = ("kv_1", "kv_0")
KV_TP = ("kv_0", "kv_1", "tp")
DP_KV = ("dp", "kv_0", "kv_1")
F32 = jnp.float32
BF16 = jnp.bfloat16
LANES = 128
NZ = 16
NY = 4
SEQS = NZ * NY
INTERPRET = False

VMEM = pl.BlockSpec(memory_space=pltpu.VMEM)
PARAMS = pltpu.CompilerParams(vmem_limit_bytes=32 * 1024 * 1024)


def kernel_call(body, out_shape, n_in, scratch=(), name=None):
    single = not isinstance(out_shape, (list, tuple))
    return pl.pallas_call(
        body,
        out_shape=out_shape,
        in_specs=[VMEM] * n_in,
        out_specs=VMEM if single else [VMEM] * len(out_shape),
        scratch_shapes=list(scratch),
        compiler_params=PARAMS,
        interpret=INTERPRET,
        name=name,
    )


def sds(shape, dtype):
    return jax.ShapeDtypeStruct(shape, dtype)


def far_z(z):
    return z // (NZ // 2)


ALL_GROUPS = [
    [(z * NY + y) * 2 + (t ^ far_z(z)) for z in range(NZ) for y in range(NY)] for t in range(2)
]


def rows_of(s):
    return (s % NY) * NZ + s // NY


def perm_matrix(dtype):
    d = lax.broadcasted_iota(jnp.int32, (SEQS, SEQS), 0)
    s = lax.broadcasted_iota(jnp.int32, (SEQS, SEQS), 1)
    return (d == rows_of(s)).astype(F32).astype(dtype)


def mm(a, b, ca, cb):
    return lax.dot_general(a, b, (((ca,), (cb,)), ((), ())), preferred_element_type=F32)


def project_kernel(
    tok_hbm, position_hbm, wq, wk, wv, wg, out_hbm, turns, tok, position, weights, out, sems, out_sems
):
    sources = (wq, wk, wv, wg)
    count = len(sources)
    width = weights.shape[2]
    copies = [pltpu.make_async_copy(tok_hbm, tok, sems.at[count])]
    for i, w in enumerate(sources):
        copies.append(pltpu.make_async_copy(w, weights.at[i], sems.at[i]))
    for copy in copies:
        copy.start()
    where = pltpu.make_async_copy(position_hbm, position, sems.at[count + 1])
    where.start()
    where.wait()
    dim = turns.shape[1]
    lane = lax.broadcasted_iota(jnp.int32, (1, dim), 1)
    power = (lane % (dim // 2)).astype(F32) / (dim // 2)
    angle = position[0].astype(F32) * jnp.exp(power * -math.log(10000.0))
    turns[0:1, :] = jnp.cos(angle)
    sine = jnp.sin(angle)
    turns[1:2, :] = jnp.where(lane < dim // 2, -sine, sine)
    copies[0].wait()
    rows = mm(perm_matrix(BF16), tok[...], 1, 0).astype(BF16)
    sends = []
    for i in range(count):
        copies[1 + i].wait()
        out[i] = mm(rows, weights[i], 1, 0).astype(BF16).reshape(NY, NZ, width)
        cols = pl.ds(i * width, width)
        sends.append(pltpu.make_async_copy(out.at[i], out_hbm.at[:, :, cols], out_sems.at[i]))
        sends[i].start()
    for send in sends:
        send.wait()


def near_sum_kernel(x, out, wide):
    for c in range(wide.shape[1]):
        cols = slice(c * LANES, (c + 1) * LANES)
        total = x[0, :, cols].astype(F32)
        for y in range(1, NY):
            total += x[y, :, cols].astype(F32)
        wide[:, c, :] = total
    out[...] = wide[...].astype(BF16)


def retention_kernel(x, turns, state, new_state, out):
    heads, dim = state.shape[1], state.shape[2]
    cosine = turns[0:1, :]
    sine = turns[1:2, :]
    line = lax.broadcasted_iota(jnp.int32, (heads, dim), 0) + lax.axis_index("tp") * heads
    decay = 1.0 - jnp.exp2(-5.0 - 6.0 * line.astype(F32) / (2 * heads - 1))
    total = x[0].astype(F32)
    for z in range(1, NZ):
        total += x[z].astype(F32)
    query = total[0:heads]
    key = total[heads : 2 * heads]
    value = total[2 * heads : 3 * heads]
    gate = total[3 * heads : 4 * heads]
    query = query * cosine + pltpu.roll(query, dim // 2, 1) * sine
    key = (key * cosine + pltpu.roll(key, dim // 2, 1) * sine) * dim ** (-0.5)
    query_t = query.T
    key_t = key.T
    lines = []
    for h in range(heads):
        updated = decay[h : h + 1, :] * state[0, h] + key_t[:, h : h + 1] * value[h : h + 1, :]
        new_state[0, h] = updated
        lines.append(jnp.sum(query_t[:, h : h + 1] * updated, axis=0, keepdims=True))
    retained = jnp.concatenate(lines, axis=0)
    mean = jnp.mean(retained, -1, keepdims=True)
    var = jnp.mean(jnp.square(retained - mean), -1, keepdims=True)
    normed = (retained - mean) * lax.rsqrt(var + 1e-05)
    silu = gate / (1.0 + jnp.exp(-gate))
    attended = (normed * silu).astype(BF16)
    out[...] = jnp.broadcast_to(attended[None], out.shape)


def mix_kernel(x, w_t, tok, out, wide):
    tp = lax.axis_index("tp")
    tps, seqs, heads, dim = x.shape
    cols = w_t.shape[0]
    groups = LANES // cols
    wide[...] = x[...].astype(F32)
    own = lax.broadcasted_iota(jnp.int32, (tok.shape[1], LANES), 0)
    lane = lax.broadcasted_iota(jnp.int32, (tok.shape[1], LANES), 1)
    pick = (own == tp * cols + lane % cols).astype(F32).astype(BF16)
    rows = mm(perm_matrix(BF16), tok[...], 1, 0).astype(BF16)
    acc = mm(rows, pick, 1, 0)
    w4 = jnp.concatenate([w_t[...]] * groups, axis=0)
    for t in range(tps):
        for h in range(heads):
            k = (t * heads + h) * dim
            acc += mm(wide[t, :, h, :].astype(BF16), w4[:, k : k + dim], 1, 1)
    per = seqs // groups
    turn = (lax.axis_index("kv_1") % (groups // tps)) * tps + tp
    block = lax.broadcasted_iota(jnp.int32, (per, LANES), 1) // cols
    block = (block + groups - turn) % groups
    packed = acc[0:per]
    for g in range(1, groups):
        packed = jnp.where(block == g, acc[g * per : (g + 1) * per], packed)
    out[...] = jnp.broadcast_to(packed.astype(BF16)[None], out.shape)


def feed_kernel(
    x, gain, wg_t, wu_t, wd, state, own, other, row, state_out, wide, narrow, stats, sem
):
    keep = pltpu.make_async_copy(state, state_out, sem)
    keep.start()
    tps = x.shape[0]
    per = x.shape[3]
    tp = lax.axis_index("tp")
    place = lax.axis_index("kv_1") * NZ + lax.axis_index("kv_0")
    groups = SEQS // per
    cols = LANES // groups
    chips = groups // tps
    width = wide.shape[1]
    lane = lax.broadcasted_iota(jnp.int32, (per, LANES), 1) // cols
    sums = [jnp.zeros((per, LANES), F32) for _ in range(groups)]
    squares = [jnp.zeros((per, LANES), F32) for _ in range(groups)]
    for a in range(SEQS // chips):
        sources = []
        for q in range(groups):
            kv = a * chips + q // tps
            sources.append(x[q % tps, kv % NY, kv // NY].astype(F32))
        for g in range(groups):
            tile = sources[(groups - g) % groups]
            for j in range(1, groups):
                tile = jnp.where(lane == j, sources[(j - g) % groups], tile)
            if g:
                tile = pltpu.roll(tile, LANES - g * cols, 1)
            wide[g * per : (g + 1) * per, a * LANES : (a + 1) * LANES] = tile
            sums[g] += tile
            squares[g] += tile * tile
    mean = jnp.sum(jnp.concatenate(sums, 0), -1, keepdims=True) / width
    var = jnp.sum(jnp.concatenate(squares, 0), -1, keepdims=True) / width - mean * mean
    scale = lax.rsqrt(var + 1e-05)
    stats[0] = jnp.broadcast_to(mean, stats.shape[1:])
    stats[1] = jnp.broadcast_to(scale, stats.shape[1:])
    for a in range(width // LANES):
        c = slice(a * LANES, (a + 1) * LANES)
        narrow[:, c] = ((wide[:, c] - mean) * scale * gain[:, c]).astype(BF16)
    own_mean = stats[0, pl.ds(place, 1), 0:1]
    own_scale = stats[1, pl.ds(place, 1), 0:1]
    own_row = (wide[pl.ds(place, 1), :] - own_mean) * own_scale * gain[...]
    row[...] = own_row.astype(BF16).astype(F32)
    gate = mm(narrow[...], wg_t[...], 1, 1)
    up = mm(narrow[...], wu_t[...], 1, 1)
    inner = (gate / (1.0 + jnp.exp(-gate)) * up).astype(BF16)
    half = own.shape[1]
    step = 4 * LANES
    for c in range(0, half, step):
        mine = pl.multiple_of(tp * half + c, step)
        theirs = pl.multiple_of((1 - tp) * half + c, step)
        own[:, c : c + step] = mm(inner, wd[:, pl.ds(mine, step)], 1, 0).astype(BF16)
        other[:, c : c + step] = mm(inner, wd[:, pl.ds(theirs, step)], 1, 0).astype(BF16)
    keep.wait()


def pair_sum_kernel(own, both, out):
    tp = lax.axis_index("tp")
    out[...] = (own[...].astype(F32) + both[1 - tp].astype(F32)).astype(BF16)


def ffn_sum_kernel(x, hidden, out):
    per = x.shape[1]
    tp = lax.axis_index("tp")
    total = hidden[pl.ds(pl.multiple_of(tp * per, per), per), :]
    for d in range(x.shape[0]):
        total += x[d].astype(F32)
    out[...] = total


def total_of(x):
    return jnp.sum(jnp.sum(x, 0, keepdims=True), 1, keepdims=True)


def final_norm_kernel(x, gain, out):
    p = x[...]
    count = p.shape[0] * p.shape[1]
    mean = total_of(p) / count
    var = total_of(p * p) / count - mean * mean
    normed = ((p - mean) * lax.rsqrt(var + 1e-05) * gain[...]).astype(BF16)
    lines = p.shape[0]
    d = lax.broadcasted_iota(jnp.int32, (SEQS, lines), 0)
    line = lax.broadcasted_iota(jnp.int32, (SEQS, lines), 1)
    spread = (d * lines // SEQS == line).astype(F32).astype(BF16)
    out[...] = mm(spread, normed, 1, 0)


def place_kernel(x, out):
    cols = out.shape[0]
    offset = (lax.axis_index("kv_1") % 2) * (2 * cols) + lax.axis_index("tp") * cols
    col = lax.broadcasted_iota(jnp.int32, (cols, LANES), 0)
    lane = lax.broadcasted_iota(jnp.int32, (cols, LANES), 1)
    pick = (lane == col + offset).astype(F32).astype(BF16)
    out[...] = mm(pick, x[...].astype(BF16), 1, 1).astype(BF16)


def on_device(
    tokens,
    positions,
    state,
    w_query,
    w_key,
    w_value,
    w_gate,
    w_out,
    gain_mix,
    w_ffn_gate,
    w_ffn_up,
    w_ffn_down,
    gain_out,
):
    heads, dim = state.shape[1], state.shape[2]
    width = w_ffn_gate.shape[0]
    cols = w_out.shape[1]
    proj = 4 * heads
    half = width // 2
    tp = lax.axis_index("tp")

    parts, turns = pl.pallas_call(
        project_kernel,
        out_shape=[sds((NY, NZ, proj * dim), BF16), sds((2, dim), F32)],
        in_specs=[pl.BlockSpec(memory_space=pl.ANY)] * 6,
        out_specs=[pl.BlockSpec(memory_space=pl.ANY), VMEM],
        scratch_shapes=[
            pltpu.VMEM(tokens.shape, BF16),
            pltpu.SMEM((1,), jnp.int32),
            pltpu.VMEM((4, *w_query.shape), BF16),
            pltpu.VMEM((4, NY, NZ, w_query.shape[1]), BF16),
            pltpu.SemaphoreType.DMA((6,)),
            pltpu.SemaphoreType.DMA((4,)),
        ],
        interpret=INTERPRET,
        name="project",
    )(tokens, positions, w_query, w_key, w_value, w_gate)
    near = lax.all_to_all(parts, "kv_1", 0, 0, tiled=True)
    near = kernel_call(
        near_sum_kernel,
        sds((NZ, proj, dim), BF16),
        1,
        scratch=[pltpu.VMEM((NZ, proj, dim), F32)],
        name="near_sum",
    )(near)
    far = lax.all_to_all(near, "kv_0", 0, 0, tiled=True)
    updated, attended = kernel_call(
        retention_kernel,
        [sds(state.shape, F32), sds((SEQS, heads, dim), BF16)],
        3,
        name="retention",
    )(far, turns, state)
    gathered = lax.all_to_all(attended, YZ, 0, 0, tiled=True)
    gathered = lax.all_gather(gathered, "tp", axis=0)
    per = SEQS * cols // LANES
    mixed = kernel_call(
        mix_kernel,
        sds((NZ, per, LANES), BF16),
        3,
        scratch=[pltpu.VMEM((2, SEQS, heads, dim), F32)],
        name="mix",
    )(gathered.reshape(2, SEQS, heads, dim), w_out.T, tokens)
    rows = lax.all_to_all(mixed, "kv_0", 0, 0, tiled=True)
    rows = jnp.broadcast_to(rows[None], (NY, *rows.shape))
    rows = lax.all_to_all(rows, "kv_1", 0, 0, tiled=True)
    rows = lax.all_gather(rows, "tp", axis=0)
    lines = half // LANES
    own, other, hidden_row, new_state = pl.pallas_call(
        feed_kernel,
        out_shape=[
            sds((SEQS, half), BF16),
            sds((SEQS, half), BF16),
            sds((1, width), F32),
            sds(state.shape, F32),
        ],
        in_specs=[VMEM] * 6,
        out_specs=[VMEM] * 3 + [pl.BlockSpec(memory_space=pl.ANY)],
        scratch_shapes=[
            pltpu.VMEM((SEQS, width), F32),
            pltpu.VMEM((SEQS, width), BF16),
            pltpu.VMEM((2, SEQS, LANES), F32),
            pltpu.SemaphoreType.DMA,
        ],
        compiler_params=PARAMS,
        interpret=INTERPRET,
        name="feed",
    )(rows, gain_mix[None, :], w_ffn_gate.T, w_ffn_up.T, w_ffn_down, updated)
    both = lax.all_gather(other, "tp", axis=0)
    part = kernel_call(pair_sum_kernel, sds(own.shape, BF16), 2, name="pair_sum")(own, both)
    part = lax.all_to_all(part.reshape(NY, NZ, half), "kv_1", 0, 0, tiled=True)
    part = kernel_call(
        near_sum_kernel,
        sds((NZ, lines, LANES), BF16),
        1,
        scratch=[pltpu.VMEM((NZ, lines, LANES), F32)],
        name="half_sum",
    )(part)
    part = lax.all_to_all(part, "kv_0", 0, 0, tiled=True)
    summed = kernel_call(ffn_sum_kernel, sds((lines, LANES), F32), 2, name="ffn_sum")(
        part, hidden_row.reshape(2 * lines, LANES)
    )
    summed = lax.all_gather(summed, "tp", axis=0, tiled=True)
    spread = kernel_call(final_norm_kernel, sds((SEQS, LANES), F32), 2, name="final_norm")(
        summed, gain_out.reshape(2 * lines, LANES)
    )
    spread = lax.all_to_all(
        spread.reshape(SEQS, 1, LANES), KV_TP, 0, 0, tiled=True, axis_index_groups=ALL_GROUPS
    )
    layer_out = kernel_call(place_kernel, sds((cols, SEQS), BF16), 1, name="place")(
        spread.reshape(SEQS, LANES)
    )
    return (layer_out.T, new_state)


def solution(mesh):
    finer = Mesh(
        mesh.devices.reshape(mesh.shape["dp"], NZ, NY, mesh.shape["tp"]),
        ("dp", "kv_0", "kv_1", "tp"),
    )
    return jax.shard_map(
        on_device,
        mesh=finer,
        in_specs=(
            P("dp", KV),
            P(DP_KV),
            P(DP_KV, "tp", None, None),
            P(KV, "tp"),
            P(KV, "tp"),
            P(KV, "tp"),
            P(KV, "tp"),
            P(None, KV_TP),
            P(),
            P(None, KV_TP),
            P(None, KV_TP),
            P(KV_TP, None),
            P(),
        ),
        out_specs=(P("dp", KV_TP), P(DP_KV, "tp", None, None)),
        check_vma=False,
    )
```

```python
import math

import jax
import jax.numpy as jnp
from jax import lax
from jax.experimental import pallas as pl
from jax.experimental.pallas import tpu as pltpu
from jax.sharding import Mesh
from jax.sharding import PartitionSpec as P

KV = ("kv_0", "kv_1")
YZ = ("kv_1", "kv_0")
KV_TP = ("kv_0", "kv_1", "tp")
DP_KV = ("dp", "kv_0", "kv_1")
F32 = jnp.float32
BF16 = jnp.bfloat16
LANES = 128
NZ = 16
NY = 4
SEQS = NZ * NY
INTERPRET = False

VMEM = pl.BlockSpec(memory_space=pltpu.VMEM)
PARAMS = pltpu.CompilerParams(vmem_limit_bytes=32 * 1024 * 1024)


def kernel_call(body, out_shape, n_in, scratch=(), name=None):
    single = not isinstance(out_shape, (list, tuple))
    return pl.pallas_call(
        body,
        out_shape=out_shape,
        in_specs=[VMEM] * n_in,
        out_specs=VMEM if single else [VMEM] * len(out_shape),
        scratch_shapes=list(scratch),
        compiler_params=PARAMS,
        interpret=INTERPRET,
        name=name,
    )


def in_hbm(x):
    return pltpu.with_memory_space_constraint(x, pltpu.HBM)


def sds(shape, dtype):
    return jax.ShapeDtypeStruct(shape, dtype)


def far_z(z):
    return z // (NZ // 2)


ALL_GROUPS = [
    [(z * NY + y) * 2 + (t ^ far_z(z)) for z in range(NZ) for y in range(NY)] for t in range(2)
]


def rows_of(s):
    return (s % NY) * NZ + s // NY


def perm_matrix(dtype):
    d = lax.broadcasted_iota(jnp.int32, (SEQS, SEQS), 0)
    s = lax.broadcasted_iota(jnp.int32, (SEQS, SEQS), 1)
    return (d == rows_of(s)).astype(F32).astype(dtype)


def mm(a, b, ca, cb):
    return lax.dot_general(a, b, (((ca,), (cb,)), ((), ())), preferred_element_type=F32)


def project_kernel(position, tok_hbm, wq, wk, wv, wg, out, tok, weights, sems):
    sources = (wq, wk, wv, wg)
    count = len(sources)
    width = weights.shape[2]
    copies = [pltpu.make_async_copy(tok_hbm, tok, sems.at[count])]
    for i, w in enumerate(sources):
        copies.append(pltpu.make_async_copy(w, weights.at[i], sems.at[i]))
    for copy in copies:
        copy.start()
    copies[0].wait()
    rows = mm(perm_matrix(BF16), tok[...], 1, 0).astype(BF16)
    for i in range(count):
        copies[1 + i].wait()
        part = mm(rows, weights[i], 1, 0).astype(BF16)
        out[:, :, i * width : (i + 1) * width] = part.reshape(NY, NZ, width)


def near_sum_kernel(x, out, wide):
    for c in range(wide.shape[1]):
        cols = slice(c * LANES, (c + 1) * LANES)
        total = x[0, :, cols].astype(F32)
        for y in range(1, NY):
            total += x[y, :, cols].astype(F32)
        wide[:, c, :] = total
    out[...] = wide[...].astype(BF16)


def first_sum_kernel(position, x, out, turns, wide):
    dim = turns.shape[1]
    lane = lax.broadcasted_iota(jnp.int32, (1, dim), 1)
    power = (lane % (dim // 2)).astype(F32) / (dim // 2)
    angle = position[0].astype(F32) * jnp.exp(power * -math.log(10000.0))
    turns[0:1, :] = jnp.cos(angle)
    sine = jnp.sin(angle)
    turns[1:2, :] = jnp.where(lane < dim // 2, -sine, sine)
    near_sum_kernel(x, out, wide)


def retention_kernel(x, turns, state, new_state, out):
    heads, dim = state.shape[1], state.shape[2]
    cosine = turns[0:1, :]
    sine = turns[1:2, :]
    line = lax.broadcasted_iota(jnp.int32, (heads, dim), 0) + lax.axis_index("tp") * heads
    decay = 1.0 - jnp.exp2(-5.0 - 6.0 * line.astype(F32) / (2 * heads - 1))
    total = x[0].astype(F32)
    for z in range(1, NZ):
        total += x[z].astype(F32)
    query = total[0:heads]
    key = total[heads : 2 * heads]
    value = total[2 * heads : 3 * heads]
    gate = total[3 * heads : 4 * heads]
    query = query * cosine + pltpu.roll(query, dim // 2, 1) * sine
    key = (key * cosine + pltpu.roll(key, dim // 2, 1) * sine) * dim ** (-0.5)
    query_t = query.T
    key_t = key.T
    lines = []
    for h in range(heads):
        updated = decay[h : h + 1, :] * state[0, h] + key_t[:, h : h + 1] * value[h : h + 1, :]
        new_state[0, h] = updated
        lines.append(jnp.sum(query_t[:, h : h + 1] * updated, axis=0, keepdims=True))
    retained = jnp.concatenate(lines, axis=0)
    mean = jnp.mean(retained, -1, keepdims=True)
    var = jnp.mean(jnp.square(retained - mean), -1, keepdims=True)
    normed = (retained - mean) * lax.rsqrt(var + 1e-05)
    silu = gate / (1.0 + jnp.exp(-gate))
    attended = (normed * silu).astype(BF16)
    out[...] = jnp.broadcast_to(attended[None], out.shape)


def mix_kernel(x, w_t, tok, out, wide):
    tp = lax.axis_index("tp")
    tps, seqs, heads, dim = x.shape
    cols = w_t.shape[0]
    groups = LANES // cols
    wide[...] = x[...].astype(F32)
    own = lax.broadcasted_iota(jnp.int32, (tok.shape[1], LANES), 0)
    lane = lax.broadcasted_iota(jnp.int32, (tok.shape[1], LANES), 1)
    pick = (own == tp * cols + lane % cols).astype(F32).astype(BF16)
    rows = mm(perm_matrix(BF16), tok[...], 1, 0).astype(BF16)
    acc = mm(rows, pick, 1, 0)
    w4 = jnp.concatenate([w_t[...]] * groups, axis=0)
    for t in range(tps):
        for h in range(heads):
            k = (t * heads + h) * dim
            acc += mm(wide[t, :, h, :].astype(BF16), w4[:, k : k + dim], 1, 1)
    per = seqs // groups
    turn = (lax.axis_index("kv_1") % (groups // tps)) * tps + tp
    block = lax.broadcasted_iota(jnp.int32, (per, LANES), 1) // cols
    block = (block + groups - turn) % groups
    packed = acc[0:per]
    for g in range(1, groups):
        packed = jnp.where(block == g, acc[g * per : (g + 1) * per], packed)
    out[...] = jnp.broadcast_to(packed.astype(BF16)[None], out.shape)


def feed_kernel(
    x, gain, wg_t, wu_t, wd, state, own, other, row, state_out, wide, narrow, stats, sem
):
    keep = pltpu.make_async_copy(state, state_out, sem)
    keep.start()
    tps = x.shape[0]
    per = x.shape[3]
    tp = lax.axis_index("tp")
    place = lax.axis_index("kv_1") * NZ + lax.axis_index("kv_0")
    groups = SEQS // per
    cols = LANES // groups
    chips = groups // tps
    width = wide.shape[1]
    lane = lax.broadcasted_iota(jnp.int32, (per, LANES), 1) // cols
    sums = [jnp.zeros((per, LANES), F32) for _ in range(groups)]
    squares = [jnp.zeros((per, LANES), F32) for _ in range(groups)]
    for a in range(SEQS // chips):
        sources = []
        for q in range(groups):
            kv = a * chips + q // tps
            sources.append(x[q % tps, kv % NY, kv // NY].astype(F32))
        for g in range(groups):
            tile = sources[(groups - g) % groups]
            for j in range(1, groups):
                tile = jnp.where(lane == j, sources[(j - g) % groups], tile)
            if g:
                tile = pltpu.roll(tile, LANES - g * cols, 1)
            wide[g * per : (g + 1) * per, a * LANES : (a + 1) * LANES] = tile
            sums[g] += tile
            squares[g] += tile * tile
    mean = jnp.sum(jnp.concatenate(sums, 0), -1, keepdims=True) / width
    var = jnp.sum(jnp.concatenate(squares, 0), -1, keepdims=True) / width - mean * mean
    scale = lax.rsqrt(var + 1e-05)
    stats[0] = jnp.broadcast_to(mean, stats.shape[1:])
    stats[1] = jnp.broadcast_to(scale, stats.shape[1:])
    for a in range(width // LANES):
        c = slice(a * LANES, (a + 1) * LANES)
        narrow[:, c] = ((wide[:, c] - mean) * scale * gain[:, c]).astype(BF16)
    own_mean = stats[0, pl.ds(place, 1), 0:1]
    own_scale = stats[1, pl.ds(place, 1), 0:1]
    own_row = (wide[pl.ds(place, 1), :] - own_mean) * own_scale * gain[...]
    row[...] = own_row.astype(BF16).astype(F32)
    gate = mm(narrow[...], wg_t[...], 1, 1)
    up = mm(narrow[...], wu_t[...], 1, 1)
    inner = (gate / (1.0 + jnp.exp(-gate)) * up).astype(BF16)
    half = own.shape[1]
    step = 4 * LANES
    for c in range(0, half, step):
        mine = pl.multiple_of(tp * half + c, step)
        theirs = pl.multiple_of((1 - tp) * half + c, step)
        own[:, c : c + step] = mm(inner, wd[:, pl.ds(mine, step)], 1, 0).astype(BF16)
        other[:, c : c + step] = mm(inner, wd[:, pl.ds(theirs, step)], 1, 0).astype(BF16)
    keep.wait()


def pair_sum_kernel(own, both, out):
    tp = lax.axis_index("tp")
    out[...] = (own[...].astype(F32) + both[1 - tp].astype(F32)).astype(BF16)


def ffn_sum_kernel(x, hidden, out):
    per = x.shape[1]
    tp = lax.axis_index("tp")
    total = hidden[pl.ds(pl.multiple_of(tp * per, per), per), :]
    for d in range(x.shape[0]):
        total += x[d].astype(F32)
    out[...] = total


def total_of(x):
    return jnp.sum(jnp.sum(x, 0, keepdims=True), 1, keepdims=True)


def final_norm_kernel(x, gain, out):
    p = x[...]
    count = p.shape[0] * p.shape[1]
    mean = total_of(p) / count
    var = total_of(p * p) / count - mean * mean
    normed = ((p - mean) * lax.rsqrt(var + 1e-05) * gain[...]).astype(BF16)
    lines = p.shape[0]
    d = lax.broadcasted_iota(jnp.int32, (SEQS, lines), 0)
    line = lax.broadcasted_iota(jnp.int32, (SEQS, lines), 1)
    spread = (d * lines // SEQS == line).astype(F32).astype(BF16)
    out[...] = mm(spread, normed, 1, 0)


def place_kernel(x, out):
    cols = out.shape[0]
    offset = (lax.axis_index("kv_1") % 2) * (2 * cols) + lax.axis_index("tp") * cols
    col = lax.broadcasted_iota(jnp.int32, (cols, LANES), 0)
    lane = lax.broadcasted_iota(jnp.int32, (cols, LANES), 1)
    pick = (lane == col + offset).astype(F32).astype(BF16)
    out[...] = mm(pick, x[...].astype(BF16), 1, 1).astype(BF16)


def on_device(
    tokens,
    positions,
    state,
    w_query,
    w_key,
    w_value,
    w_gate,
    w_out,
    gain_mix,
    w_ffn_gate,
    w_ffn_up,
    w_ffn_down,
    gain_out,
):
    heads, dim = state.shape[1], state.shape[2]
    width = w_ffn_gate.shape[0]
    cols = w_out.shape[1]
    proj = 4 * heads
    half = width // 2
    tp = lax.axis_index("tp")

    smem = pl.BlockSpec(memory_space=pltpu.SMEM)
    parts = pl.pallas_call(
        project_kernel,
        out_shape=sds((NY, NZ, proj * dim), BF16),
        in_specs=[smem] + [pl.BlockSpec(memory_space=pl.ANY)] * 5,
        out_specs=VMEM,
        scratch_shapes=[
            pltpu.VMEM(tokens.shape, BF16),
            pltpu.VMEM((4, *w_query.shape), BF16),
            pltpu.SemaphoreType.DMA((5,)),
        ],
        compiler_params=PARAMS,
        interpret=INTERPRET,
        name="project",
    )(positions, *map(in_hbm, (tokens, w_query, w_key, w_value, w_gate)))
    near = lax.all_to_all(parts, "kv_1", 0, 0, tiled=True)
    near, turns = pl.pallas_call(
        first_sum_kernel,
        out_shape=[sds((NZ, proj, dim), BF16), sds((2, dim), F32)],
        in_specs=[smem, VMEM],
        out_specs=[VMEM, VMEM],
        scratch_shapes=[pltpu.VMEM((NZ, proj, dim), F32)],
        compiler_params=PARAMS,
        interpret=INTERPRET,
        name="near_sum",
    )(positions, near)
    far = lax.all_to_all(near, "kv_0", 0, 0, tiled=True)
    updated, attended = kernel_call(
        retention_kernel,
        [sds(state.shape, F32), sds((SEQS, heads, dim), BF16)],
        3,
        name="retention",
    )(far, turns, state)
    gathered = lax.all_to_all(attended, YZ, 0, 0, tiled=True)
    gathered = lax.all_gather(gathered, "tp", axis=0)
    per = SEQS * cols // LANES
    mixed = kernel_call(
        mix_kernel,
        sds((NZ, per, LANES), BF16),
        3,
        scratch=[pltpu.VMEM((2, SEQS, heads, dim), F32)],
        name="mix",
    )(gathered.reshape(2, SEQS, heads, dim), w_out.T, tokens)
    rows = lax.all_to_all(mixed, "kv_0", 0, 0, tiled=True)
    rows = jnp.broadcast_to(rows[None], (NY, *rows.shape))
    rows = lax.all_to_all(rows, "kv_1", 0, 0, tiled=True)
    rows = lax.all_gather(rows, "tp", axis=0)
    lines = half // LANES
    own, other, hidden_row, new_state = pl.pallas_call(
        feed_kernel,
        out_shape=[
            sds((SEQS, half), BF16),
            sds((SEQS, half), BF16),
            sds((1, width), F32),
            sds(state.shape, F32),
        ],
        in_specs=[VMEM] * 6,
        out_specs=[VMEM] * 3 + [pl.BlockSpec(memory_space=pl.ANY)],
        scratch_shapes=[
            pltpu.VMEM((SEQS, width), F32),
            pltpu.VMEM((SEQS, width), BF16),
            pltpu.VMEM((2, SEQS, LANES), F32),
            pltpu.SemaphoreType.DMA,
        ],
        compiler_params=PARAMS,
        interpret=INTERPRET,
        name="feed",
    )(rows, gain_mix[None, :], w_ffn_gate.T, w_ffn_up.T, w_ffn_down, updated)
    both = lax.all_gather(other, "tp", axis=0)
    part = kernel_call(pair_sum_kernel, sds(own.shape, BF16), 2, name="pair_sum")(own, both)
    part = lax.all_to_all(part.reshape(NY, NZ, half), "kv_1", 0, 0, tiled=True)
    part = kernel_call(
        near_sum_kernel,
        sds((NZ, lines, LANES), BF16),
        1,
        scratch=[pltpu.VMEM((NZ, lines, LANES), F32)],
        name="half_sum",
    )(part)
    part = lax.all_to_all(part, "kv_0", 0, 0, tiled=True)
    summed = kernel_call(ffn_sum_kernel, sds((lines, LANES), F32), 2, name="ffn_sum")(
        part, hidden_row.reshape(2 * lines, LANES)
    )
    summed = lax.all_gather(summed, "tp", axis=0, tiled=True)
    spread = kernel_call(final_norm_kernel, sds((SEQS, LANES), F32), 2, name="final_norm")(
        summed, gain_out.reshape(2 * lines, LANES)
    )
    spread = lax.all_to_all(
        spread.reshape(SEQS, 1, LANES), KV_TP, 0, 0, tiled=True, axis_index_groups=ALL_GROUPS
    )
    layer_out = kernel_call(place_kernel, sds((cols, SEQS), BF16), 1, name="place")(
        spread.reshape(SEQS, LANES)
    )
    return (layer_out.T, new_state)


def solution(mesh):
    finer = Mesh(
        mesh.devices.reshape(mesh.shape["dp"], NZ, NY, mesh.shape["tp"]),
        ("dp", "kv_0", "kv_1", "tp"),
    )
    return jax.shard_map(
        on_device,
        mesh=finer,
        in_specs=(
            P("dp", KV),
            P(DP_KV),
            P(DP_KV, "tp", None, None),
            P(KV, "tp"),
            P(KV, "tp"),
            P(KV, "tp"),
            P(KV, "tp"),
            P(None, KV_TP),
            P(),
            P(None, KV_TP),
            P(None, KV_TP),
            P(KV_TP, None),
            P(),
        ),
        out_specs=(P("dp", KV_TP), P(DP_KV, "tp", None, None)),
        check_vma=False,
    )
```

```python
import math

import jax
import jax.numpy as jnp
from jax import lax
from jax.experimental import pallas as pl
from jax.experimental.pallas import tpu as pltpu
from jax.sharding import Mesh
from jax.sharding import PartitionSpec as P

KV = ("kv_0", "kv_1")
Z_TP = ("kv_0", "tp")
KV_TP = ("kv_0", "kv_1", "tp")
DP_KV = ("dp", "kv_0", "kv_1")
F32 = jnp.float32
BF16 = jnp.bfloat16
LANES = 128
NZ = 16
NY = 4
SEQS = NZ * NY
INTERPRET = False

VMEM = pl.BlockSpec(memory_space=pltpu.VMEM)
PARAMS = pltpu.CompilerParams(vmem_limit_bytes=32 * 1024 * 1024)


def kernel_call(body, out_shape, n_in, scratch=(), name=None):
    single = not isinstance(out_shape, (list, tuple))
    return pl.pallas_call(
        body,
        out_shape=out_shape,
        in_specs=[VMEM] * n_in,
        out_specs=VMEM if single else [VMEM] * len(out_shape),
        scratch_shapes=list(scratch),
        compiler_params=PARAMS,
        interpret=INTERPRET,
        name=name,
    )


def in_hbm(x):
    return pltpu.with_memory_space_constraint(x, pltpu.HBM)


def sds(shape, dtype):
    return jax.ShapeDtypeStruct(shape, dtype)


def far_z(z):
    return z // (NZ // 2)


ALL_GROUPS = [
    [(z * NY + y) * 2 + (t ^ far_z(z)) for z in range(NZ) for y in range(NY)] for t in range(2)
]


def spot(z):
    return (7 * z) % NZ


Z_GROUPS = [[spot(i) * 2 + t for i in range(NZ)] for t in range(2)]
YZ_GROUPS = [[(spot(i) * NY + y) * 2 + t for y in range(NY) for i in range(NZ)] for t in range(2)]


def along_z(x):
    return lax.all_to_all(x, Z_TP, 0, 0, tiled=True, axis_index_groups=Z_GROUPS)


def rows_of(s):
    return (s % NY) * NZ + spot(s // NY)


def perm_matrix(dtype):
    d = lax.broadcasted_iota(jnp.int32, (SEQS, SEQS), 0)
    s = lax.broadcasted_iota(jnp.int32, (SEQS, SEQS), 1)
    return (d == rows_of(s)).astype(F32).astype(dtype)


def mm(a, b, ca, cb):
    return lax.dot_general(a, b, (((ca,), (cb,)), ((), ())), preferred_element_type=F32)


def project_kernel(position, tok_hbm, wq, wk, wv, wg, out, tok, weights, tok_sem, sems):
    sources = (wq, wk, wv, wg)
    count = len(sources)
    width = weights.shape[2]
    load = pltpu.make_async_copy(tok_hbm, tok, tok_sem)
    load.start()
    parts = 4
    depth = weights.shape[1] // parts
    copies = []
    for i, w in enumerate(sources):
        for j in range(parts):
            some = pl.ds(j * depth, depth)
            copy = pltpu.make_async_copy(w.at[some], weights.at[i, some], sems.at[i, j])
            copy.start()
            copies.append(copy)
    load.wait()
    rows = mm(perm_matrix(BF16), tok[...], 1, 0).astype(BF16)
    for i in range(count):
        for j in range(parts):
            copies[i * parts + j].wait()
        part = mm(rows, weights[i], 1, 0).astype(BF16)
        out[:, :, i * width : (i + 1) * width] = part.reshape(NY, NZ, width)


def near_sum_kernel(x, out, wide):
    for c in range(wide.shape[1]):
        cols = slice(c * LANES, (c + 1) * LANES)
        total = x[0, :, cols].astype(F32)
        for y in range(1, NY):
            total += x[y, :, cols].astype(F32)
        wide[:, c, :] = total
    out[...] = wide[...].astype(BF16)


def first_sum_kernel(position, x, out, turns, wide):
    dim = turns.shape[1]
    lane = lax.broadcasted_iota(jnp.int32, (1, dim), 1)
    power = (lane % (dim // 2)).astype(F32) / (dim // 2)
    angle = position[0].astype(F32) * jnp.exp(power * -math.log(10000.0))
    turns[0:1, :] = jnp.cos(angle)
    sine = jnp.sin(angle)
    turns[1:2, :] = jnp.where(lane < dim // 2, -sine, sine)
    near_sum_kernel(x, out, wide)


def retention_kernel(x, turns, state, new_state, out):
    heads, dim = state.shape[1], state.shape[2]
    cosine = turns[0:1, :]
    sine = turns[1:2, :]
    line = lax.broadcasted_iota(jnp.int32, (heads, dim), 0) + lax.axis_index("tp") * heads
    decay = 1.0 - jnp.exp2(-5.0 - 6.0 * line.astype(F32) / (2 * heads - 1))
    total = x[0].astype(F32)
    for z in range(1, NZ):
        total += x[z].astype(F32)
    query = total[0:heads]
    key = total[heads : 2 * heads]
    value = total[2 * heads : 3 * heads]
    gate = total[3 * heads : 4 * heads]
    query = query * cosine + pltpu.roll(query, dim // 2, 1) * sine
    key = (key * cosine + pltpu.roll(key, dim // 2, 1) * sine) * dim ** (-0.5)
    query_t = query.T
    key_t = key.T
    lines = []
    for h in range(heads):
        updated = decay[h : h + 1, :] * state[0, h] + key_t[:, h : h + 1] * value[h : h + 1, :]
        new_state[0, h] = updated
        lines.append(jnp.sum(query_t[:, h : h + 1] * updated, axis=0, keepdims=True))
    retained = jnp.concatenate(lines, axis=0)
    mean = jnp.mean(retained, -1, keepdims=True)
    var = jnp.mean(jnp.square(retained - mean), -1, keepdims=True)
    normed = (retained - mean) * lax.rsqrt(var + 1e-05)
    silu = gate / (1.0 + jnp.exp(-gate))
    attended = (normed * silu).astype(BF16)
    out[...] = jnp.broadcast_to(attended[None], out.shape)


def mix_kernel(x, w_t, tok, out, wide):
    tp = lax.axis_index("tp")
    tps, seqs, heads, dim = x.shape
    cols = w_t.shape[0]
    groups = LANES // cols
    wide[...] = x[...].astype(F32)
    own = lax.broadcasted_iota(jnp.int32, (tok.shape[1], LANES), 0)
    lane = lax.broadcasted_iota(jnp.int32, (tok.shape[1], LANES), 1)
    pick = (own == tp * cols + lane % cols).astype(F32).astype(BF16)
    rows = mm(perm_matrix(BF16), tok[...], 1, 0).astype(BF16)
    acc = mm(rows, pick, 1, 0)
    w4 = jnp.concatenate([w_t[...]] * groups, axis=0)
    for t in range(tps):
        for h in range(heads):
            k = (t * heads + h) * dim
            acc += mm(wide[t, :, h, :].astype(BF16), w4[:, k : k + dim], 1, 1)
    per = seqs // groups
    turn = (lax.axis_index("kv_1") % (groups // tps)) * tps + tp
    block = lax.broadcasted_iota(jnp.int32, (per, LANES), 1) // cols
    block = (block + groups - turn) % groups
    packed = acc[0:per]
    for g in range(1, groups):
        packed = jnp.where(block == g, acc[g * per : (g + 1) * per], packed)
    out[...] = jnp.broadcast_to(packed.astype(BF16)[None], out.shape)


def feed_kernel(
    x, gain, wg_t, wu_t, wd, state, own, other, row, state_out, wide, narrow, stats, sems
):
    keeps = []
    for h in range(state.shape[1]):
        keeps.append(pltpu.make_async_copy(state.at[0, h], state_out.at[0, h], sems.at[h]))
        keeps[h].start()
    tps = x.shape[0]
    per = x.shape[3]
    tp = lax.axis_index("tp")
    place = lax.axis_index("kv_1") * NZ + spot(lax.axis_index("kv_0"))
    groups = SEQS // per
    cols = LANES // groups
    chips = groups // tps
    width = wide.shape[1]
    lane = lax.broadcasted_iota(jnp.int32, (per, LANES), 1) // cols
    sums = [jnp.zeros((per, LANES), F32) for _ in range(groups)]
    squares = [jnp.zeros((per, LANES), F32) for _ in range(groups)]
    for a in range(SEQS // chips):
        sources = []
        for q in range(groups):
            kv = a * chips + q // tps
            sources.append(x[q % tps, kv % NY, spot(kv // NY)].astype(F32))
        for g in range(groups):
            tile = sources[(groups - g) % groups]
            for j in range(1, groups):
                tile = jnp.where(lane == j, sources[(j - g) % groups], tile)
            if g:
                tile = pltpu.roll(tile, LANES - g * cols, 1)
            wide[g * per : (g + 1) * per, a * LANES : (a + 1) * LANES] = tile
            sums[g] += tile
            squares[g] += tile * tile
    mean = jnp.sum(jnp.concatenate(sums, 0), -1, keepdims=True) / width
    var = jnp.sum(jnp.concatenate(squares, 0), -1, keepdims=True) / width - mean * mean
    scale = lax.rsqrt(var + 1e-05)
    stats[0] = jnp.broadcast_to(mean, stats.shape[1:])
    stats[1] = jnp.broadcast_to(scale, stats.shape[1:])
    for a in range(width // LANES):
        c = slice(a * LANES, (a + 1) * LANES)
        narrow[:, c] = ((wide[:, c] - mean) * scale * gain[:, c]).astype(BF16)
    own_mean = stats[0, pl.ds(place, 1), 0:1]
    own_scale = stats[1, pl.ds(place, 1), 0:1]
    own_row = (wide[pl.ds(place, 1), :] - own_mean) * own_scale * gain[...]
    row[...] = own_row.astype(BF16).astype(F32)
    gate = mm(narrow[...], wg_t[...], 1, 1)
    up = mm(narrow[...], wu_t[...], 1, 1)
    inner = (gate / (1.0 + jnp.exp(-gate)) * up).astype(BF16)
    half = own.shape[1]
    step = 4 * LANES
    for c in range(0, half, step):
        mine = pl.multiple_of(tp * half + c, step)
        theirs = pl.multiple_of((1 - tp) * half + c, step)
        own[:, c : c + step] = mm(inner, wd[:, pl.ds(mine, step)], 1, 0).astype(BF16)
        other[:, c : c + step] = mm(inner, wd[:, pl.ds(theirs, step)], 1, 0).astype(BF16)
    for keep in keeps:
        keep.wait()


def pair_sum_kernel(own, both, out):
    tp = lax.axis_index("tp")
    out[...] = (own[...].astype(F32) + both[1 - tp].astype(F32)).astype(BF16)


def ffn_sum_kernel(x, hidden, out):
    per = x.shape[1]
    tp = lax.axis_index("tp")
    total = hidden[pl.ds(pl.multiple_of(tp * per, per), per), :]
    for d in range(x.shape[0]):
        total += x[d].astype(F32)
    out[...] = total


def total_of(x):
    return jnp.sum(jnp.sum(x, 0, keepdims=True), 1, keepdims=True)


def final_norm_kernel(x, gain, out):
    p = x[...]
    count = p.shape[0] * p.shape[1]
    mean = total_of(p) / count
    var = total_of(p * p) / count - mean * mean
    normed = ((p - mean) * lax.rsqrt(var + 1e-05) * gain[...]).astype(BF16)
    lines = p.shape[0]
    d = lax.broadcasted_iota(jnp.int32, (SEQS, lines), 0)
    line = lax.broadcasted_iota(jnp.int32, (SEQS, lines), 1)
    spread = (d * lines // SEQS == line).astype(F32).astype(BF16)
    out[...] = mm(spread, normed, 1, 0)


def place_kernel(x, out):
    cols = out.shape[0]
    offset = (lax.axis_index("kv_1") % 2) * (2 * cols) + lax.axis_index("tp") * cols
    col = lax.broadcasted_iota(jnp.int32, (cols, LANES), 0)
    lane = lax.broadcasted_iota(jnp.int32, (cols, LANES), 1)
    pick = (lane == col + offset).astype(F32).astype(BF16)
    out[...] = mm(pick, x[...].astype(BF16), 1, 1).astype(BF16)


def on_device(
    tokens,
    positions,
    state,
    w_query,
    w_key,
    w_value,
    w_gate,
    w_out,
    gain_mix,
    w_ffn_gate,
    w_ffn_up,
    w_ffn_down,
    gain_out,
):
    heads, dim = state.shape[1], state.shape[2]
    width = w_ffn_gate.shape[0]
    cols = w_out.shape[1]
    proj = 4 * heads
    half = width // 2
    tp = lax.axis_index("tp")

    smem = pl.BlockSpec(memory_space=pltpu.SMEM)
    parts = pl.pallas_call(
        project_kernel,
        out_shape=sds((NY, NZ, proj * dim), BF16),
        in_specs=[smem] + [pl.BlockSpec(memory_space=pl.ANY)] * 5,
        out_specs=VMEM,
        scratch_shapes=[
            pltpu.VMEM(tokens.shape, BF16),
            pltpu.VMEM((4, *w_query.shape), BF16),
            pltpu.SemaphoreType.DMA,
            pltpu.SemaphoreType.DMA((4, 4)),
        ],
        compiler_params=PARAMS,
        interpret=INTERPRET,
        name="project",
    )(positions, *map(in_hbm, (tokens, w_query, w_key, w_value, w_gate)))
    near = lax.all_to_all(parts, "kv_1", 0, 0, tiled=True)
    near, turns = pl.pallas_call(
        first_sum_kernel,
        out_shape=[sds((NZ, proj, dim), BF16), sds((2, dim), F32)],
        in_specs=[smem, VMEM],
        out_specs=[VMEM, VMEM],
        scratch_shapes=[pltpu.VMEM((NZ, proj, dim), F32)],
        compiler_params=PARAMS,
        interpret=INTERPRET,
        name="near_sum",
    )(positions, near)
    far = along_z(near)
    updated, attended = kernel_call(
        retention_kernel,
        [sds(state.shape, F32), sds((SEQS, heads, dim), BF16)],
        3,
        name="retention",
    )(far, turns, state)
    gathered = lax.all_to_all(
        attended, KV_TP, 0, 0, tiled=True, axis_index_groups=YZ_GROUPS
    )
    gathered = lax.all_gather(gathered, "tp", axis=0)
    per = SEQS * cols // LANES
    mixed = kernel_call(
        mix_kernel,
        sds((NZ, per, LANES), BF16),
        3,
        scratch=[pltpu.VMEM((2, SEQS, heads, dim), F32)],
        name="mix",
    )(gathered.reshape(2, SEQS, heads, dim), w_out.T, tokens)
    rows = along_z(mixed)
    rows = jnp.broadcast_to(rows[None], (NY, *rows.shape))
    rows = lax.all_to_all(rows, "kv_1", 0, 0, tiled=True)
    rows = lax.all_gather(rows, "tp", axis=0)
    lines = half // LANES
    own, other, hidden_row, new_state = pl.pallas_call(
        feed_kernel,
        out_shape=[
            sds((SEQS, half), BF16),
            sds((SEQS, half), BF16),
            sds((1, width), F32),
            sds(state.shape, F32),
        ],
        in_specs=[VMEM] * 6,
        out_specs=[VMEM] * 3 + [pl.BlockSpec(memory_space=pl.ANY)],
        scratch_shapes=[
            pltpu.VMEM((SEQS, width), F32),
            pltpu.VMEM((SEQS, width), BF16),
            pltpu.VMEM((2, SEQS, LANES), F32),
            pltpu.SemaphoreType.DMA((heads,)),
        ],
        compiler_params=PARAMS,
        interpret=INTERPRET,
        name="feed",
    )(rows, gain_mix[None, :], w_ffn_gate.T, w_ffn_up.T, w_ffn_down, updated)
    both = lax.all_gather(other, "tp", axis=0)
    part = kernel_call(pair_sum_kernel, sds(own.shape, BF16), 2, name="pair_sum")(own, both)
    part = lax.all_to_all(part.reshape(NY, NZ, half), "kv_1", 0, 0, tiled=True)
    part = kernel_call(
        near_sum_kernel,
        sds((NZ, lines, LANES), BF16),
        1,
        scratch=[pltpu.VMEM((NZ, lines, LANES), F32)],
        name="half_sum",
    )(part)
    part = along_z(part)
    summed = kernel_call(ffn_sum_kernel, sds((lines, LANES), F32), 2, name="ffn_sum")(
        part, hidden_row.reshape(2 * lines, LANES)
    )
    summed = lax.all_gather(summed, "tp", axis=0, tiled=True)
    spread = kernel_call(final_norm_kernel, sds((SEQS, LANES), F32), 2, name="final_norm")(
        summed, gain_out.reshape(2 * lines, LANES)
    )
    spread = lax.all_to_all(
        spread.reshape(SEQS, 1, LANES), KV_TP, 0, 0, tiled=True, axis_index_groups=ALL_GROUPS
    )
    layer_out = kernel_call(place_kernel, sds((cols, SEQS), BF16), 1, name="place")(
        spread.reshape(SEQS, LANES)
    )
    return (layer_out.T, new_state)


def solution(mesh):
    finer = Mesh(
        mesh.devices.reshape(mesh.shape["dp"], NZ, NY, mesh.shape["tp"]),
        ("dp", "kv_0", "kv_1", "tp"),
    )
    return jax.shard_map(
        on_device,
        mesh=finer,
        in_specs=(
            P("dp", KV),
            P(DP_KV),
            P(DP_KV, "tp", None, None),
            P(KV, "tp"),
            P(KV, "tp"),
            P(KV, "tp"),
            P(KV, "tp"),
            P(None, KV_TP),
            P(),
            P(None, KV_TP),
            P(None, KV_TP),
            P(KV_TP, None),
            P(),
        ),
        out_specs=(P("dp", KV_TP), P(DP_KV, "tp", None, None)),
        check_vma=False,
    )
```

```python
import math

import jax
import jax.numpy as jnp
from jax import lax
from jax.experimental import pallas as pl
from jax.experimental.pallas import tpu as pltpu
from jax.sharding import Mesh
from jax.sharding import PartitionSpec as P

KV = ("kv_0", "kv_1")
Z_TP = ("kv_0", "tp")
KV_TP = ("kv_0", "kv_1", "tp")
DP_KV = ("dp", "kv_0", "kv_1")
F32 = jnp.float32
BF16 = jnp.bfloat16
LANES = 128
NZ = 16
NY = 4
SEQS = NZ * NY
INTERPRET = False

VMEM = pl.BlockSpec(memory_space=pltpu.VMEM)
PARAMS = pltpu.CompilerParams(vmem_limit_bytes=32 * 1024 * 1024)


def kernel_call(body, out_shape, n_in, scratch=(), name=None):
    single = not isinstance(out_shape, (list, tuple))
    return pl.pallas_call(
        body,
        out_shape=out_shape,
        in_specs=[VMEM] * n_in,
        out_specs=VMEM if single else [VMEM] * len(out_shape),
        scratch_shapes=list(scratch),
        compiler_params=PARAMS,
        interpret=INTERPRET,
        name=name,
    )


def in_hbm(x):
    return pltpu.with_memory_space_constraint(x, pltpu.HBM)


def sds(shape, dtype):
    return jax.ShapeDtypeStruct(shape, dtype)


def far_z(z):
    return z // (NZ // 2)


ALL_GROUPS = [
    [(z * NY + y) * 2 + (t ^ far_z(z)) for z in range(NZ) for y in range(NY)] for t in range(2)
]


def spot(z):
    return (7 * z) % NZ


Z_GROUPS = [[spot(i) * 2 + t for i in range(NZ)] for t in range(2)]


def along_z(x):
    return lax.all_to_all(x, Z_TP, 0, 0, tiled=True, axis_index_groups=Z_GROUPS)


def rows_of(s):
    return (s % NY) * NZ + spot(s // NY)


def perm_matrix(dtype):
    d = lax.broadcasted_iota(jnp.int32, (SEQS, SEQS), 0)
    s = lax.broadcasted_iota(jnp.int32, (SEQS, SEQS), 1)
    return (d == rows_of(s)).astype(F32).astype(dtype)


def mm(a, b, ca, cb):
    return lax.dot_general(a, b, (((ca,), (cb,)), ((), ())), preferred_element_type=F32)


def project_kernel(position, tok_hbm, wq, wk, wv, wg, out, tok, weights, sems):
    sources = (wq, wk, wv, wg)
    count = len(sources)
    width = weights.shape[2]
    copies = [pltpu.make_async_copy(tok_hbm, tok, sems.at[count])]
    for i, w in enumerate(sources):
        copies.append(pltpu.make_async_copy(w, weights.at[i], sems.at[i]))
    for copy in copies:
        copy.start()
    copies[0].wait()
    rows = mm(perm_matrix(BF16), tok[...], 1, 0).astype(BF16)
    for i in range(count):
        copies[1 + i].wait()
        part = mm(rows, weights[i], 1, 0).astype(BF16)
        out[:, :, i * width : (i + 1) * width] = part.reshape(NY, NZ, width)


def near_sum_kernel(x, out, wide):
    for c in range(wide.shape[1]):
        cols = slice(c * LANES, (c + 1) * LANES)
        total = x[0, :, cols].astype(F32)
        for y in range(1, NY):
            total += x[y, :, cols].astype(F32)
        wide[:, c, :] = total
    out[...] = wide[...].astype(BF16)


def first_sum_kernel(position, x, out, turns, wide):
    dim = turns.shape[1]
    lane = lax.broadcasted_iota(jnp.int32, (1, dim), 1)
    power = (lane % (dim // 2)).astype(F32) / (dim // 2)
    angle = position[0].astype(F32) * jnp.exp(power * -math.log(10000.0))
    turns[0:1, :] = jnp.cos(angle)
    sine = jnp.sin(angle)
    turns[1:2, :] = jnp.where(lane < dim // 2, -sine, sine)
    near_sum_kernel(x, out, wide)


def retention_kernel(x, turns, state, new_state, out):
    heads, dim = state.shape[1], state.shape[2]
    cosine = turns[0:1, :]
    sine = turns[1:2, :]
    line = lax.broadcasted_iota(jnp.int32, (heads, dim), 0) + lax.axis_index("tp") * heads
    decay = 1.0 - jnp.exp2(-5.0 - 6.0 * line.astype(F32) / (2 * heads - 1))
    total = x[0].astype(F32)
    for z in range(1, NZ):
        total += x[z].astype(F32)
    query = total[0:heads]
    key = total[heads : 2 * heads]
    value = total[2 * heads : 3 * heads]
    gate = total[3 * heads : 4 * heads]
    query = query * cosine + pltpu.roll(query, dim // 2, 1) * sine
    key = (key * cosine + pltpu.roll(key, dim // 2, 1) * sine) * dim ** (-0.5)
    query_t = query.T
    key_t = key.T
    lines = []
    for h in range(heads):
        updated = decay[h : h + 1, :] * state[0, h] + key_t[:, h : h + 1] * value[h : h + 1, :]
        new_state[0, h] = updated
        lines.append(jnp.sum(query_t[:, h : h + 1] * updated, axis=0, keepdims=True))
    retained = jnp.concatenate(lines, axis=0)
    mean = jnp.mean(retained, -1, keepdims=True)
    var = jnp.mean(jnp.square(retained - mean), -1, keepdims=True)
    normed = (retained - mean) * lax.rsqrt(var + 1e-05)
    silu = gate / (1.0 + jnp.exp(-gate))
    attended = (normed * silu).astype(BF16)
    out[...] = jnp.broadcast_to(attended[None], out.shape)


def mix_kernel(x, w_t, tok, out, wide):
    tp = lax.axis_index("tp")
    tps, seqs, heads, dim = x.shape
    cols = w_t.shape[0]
    groups = LANES // cols
    for t in range(tps):
        for y in range(NY):
            for z in range(NZ):
                wide[t, y * NZ + spot(z)] = x[t, y * NZ + z].astype(F32)
    own = lax.broadcasted_iota(jnp.int32, (tok.shape[1], LANES), 0)
    lane = lax.broadcasted_iota(jnp.int32, (tok.shape[1], LANES), 1)
    pick = (own == tp * cols + lane % cols).astype(F32).astype(BF16)
    rows = mm(perm_matrix(BF16), tok[...], 1, 0).astype(BF16)
    acc = mm(rows, pick, 1, 0)
    w4 = jnp.concatenate([w_t[...]] * groups, axis=0)
    for t in range(tps):
        for h in range(heads):
            k = (t * heads + h) * dim
            acc += mm(wide[t, :, h, :].astype(BF16), w4[:, k : k + dim], 1, 1)
    per = seqs // groups
    turn = (lax.axis_index("kv_1") % (groups // tps)) * tps + tp
    block = lax.broadcasted_iota(jnp.int32, (per, LANES), 1) // cols
    block = (block + groups - turn) % groups
    packed = acc[0:per]
    for g in range(1, groups):
        packed = jnp.where(block == g, acc[g * per : (g + 1) * per], packed)
    out[...] = jnp.broadcast_to(packed.astype(BF16)[None], out.shape)


def feed_kernel(
    x, gain, wg_t, wu_t, wd, state, own, other, row, state_out, wide, narrow, stats, sem
):
    keep = pltpu.make_async_copy(state, state_out, sem)
    tps = x.shape[0]
    per = x.shape[3]
    tp = lax.axis_index("tp")
    place = lax.axis_index("kv_1") * NZ + spot(lax.axis_index("kv_0"))
    groups = SEQS // per
    cols = LANES // groups
    chips = groups // tps
    width = wide.shape[1]
    lane = lax.broadcasted_iota(jnp.int32, (per, LANES), 1) // cols
    sums = [jnp.zeros((per, LANES), F32) for _ in range(groups)]
    squares = [jnp.zeros((per, LANES), F32) for _ in range(groups)]
    for a in range(SEQS // chips):
        sources = []
        for q in range(groups):
            kv = a * chips + q // tps
            sources.append(x[q % tps, kv % NY, spot(kv // NY)].astype(F32))
        for g in range(groups):
            tile = sources[(groups - g) % groups]
            for j in range(1, groups):
                tile = jnp.where(lane == j, sources[(j - g) % groups], tile)
            if g:
                tile = pltpu.roll(tile, LANES - g * cols, 1)
            wide[g * per : (g + 1) * per, a * LANES : (a + 1) * LANES] = tile
            sums[g] += tile
            squares[g] += tile * tile
    keep.start()
    mean = jnp.sum(jnp.concatenate(sums, 0), -1, keepdims=True) / width
    var = jnp.sum(jnp.concatenate(squares, 0), -1, keepdims=True) / width - mean * mean
    scale = lax.rsqrt(var + 1e-05)
    stats[0] = jnp.broadcast_to(mean, stats.shape[1:])
    stats[1] = jnp.broadcast_to(scale, stats.shape[1:])
    for a in range(width // LANES):
        c = slice(a * LANES, (a + 1) * LANES)
        narrow[:, c] = ((wide[:, c] - mean) * scale * gain[:, c]).astype(BF16)
    own_mean = stats[0, pl.ds(place, 1), 0:1]
    own_scale = stats[1, pl.ds(place, 1), 0:1]
    own_row = (wide[pl.ds(place, 1), :] - own_mean) * own_scale * gain[...]
    row[...] = own_row.astype(BF16).astype(F32)
    gate = mm(narrow[...], wg_t[...], 1, 1)
    up = mm(narrow[...], wu_t[...], 1, 1)
    inner = (gate / (1.0 + jnp.exp(-gate)) * up).astype(BF16)
    half = own.shape[1]
    step = 4 * LANES
    for c in range(0, half, step):
        mine = pl.multiple_of(tp * half + c, step)
        theirs = pl.multiple_of((1 - tp) * half + c, step)
        own[:, c : c + step] = mm(inner, wd[:, pl.ds(mine, step)], 1, 0).astype(BF16)
        other[:, c : c + step] = mm(inner, wd[:, pl.ds(theirs, step)], 1, 0).astype(BF16)
    keep.wait()


def pair_sum_kernel(own, both, out):
    tp = lax.axis_index("tp")
    out[...] = (own[...].astype(F32) + both[1 - tp].astype(F32)).astype(BF16)


def ffn_sum_kernel(x, hidden, out):
    per = x.shape[1]
    tp = lax.axis_index("tp")
    total = hidden[pl.ds(pl.multiple_of(tp * per, per), per), :]
    for d in range(x.shape[0]):
        total += x[d].astype(F32)
    out[...] = total


def total_of(x):
    return jnp.sum(jnp.sum(x, 0, keepdims=True), 1, keepdims=True)


def final_norm_kernel(x, gain, out):
    p = x[...]
    count = p.shape[0] * p.shape[1]
    mean = total_of(p) / count
    var = total_of(p * p) / count - mean * mean
    normed = ((p - mean) * lax.rsqrt(var + 1e-05) * gain[...]).astype(BF16)
    lines = p.shape[0]
    d = lax.broadcasted_iota(jnp.int32, (SEQS, lines), 0)
    line = lax.broadcasted_iota(jnp.int32, (SEQS, lines), 1)
    spread = (d * lines // SEQS == line).astype(F32).astype(BF16)
    out[...] = mm(spread, normed, 1, 0)


def place_kernel(x, out):
    cols = out.shape[0]
    offset = (lax.axis_index("kv_1") % 2) * (2 * cols) + lax.axis_index("tp") * cols
    col = lax.broadcasted_iota(jnp.int32, (cols, LANES), 0)
    lane = lax.broadcasted_iota(jnp.int32, (cols, LANES), 1)
    pick = (lane == col + offset).astype(F32).astype(BF16)
    out[...] = mm(pick, x[...].astype(BF16), 1, 1).astype(BF16)


def on_device(
    tokens,
    positions,
    state,
    w_query,
    w_key,
    w_value,
    w_gate,
    w_out,
    gain_mix,
    w_ffn_gate,
    w_ffn_up,
    w_ffn_down,
    gain_out,
):
    heads, dim = state.shape[1], state.shape[2]
    width = w_ffn_gate.shape[0]
    cols = w_out.shape[1]
    proj = 4 * heads
    half = width // 2
    tp = lax.axis_index("tp")

    smem = pl.BlockSpec(memory_space=pltpu.SMEM)
    parts = pl.pallas_call(
        project_kernel,
        out_shape=sds((NY, NZ, proj * dim), BF16),
        in_specs=[smem] + [pl.BlockSpec(memory_space=pl.ANY)] * 5,
        out_specs=VMEM,
        scratch_shapes=[
            pltpu.VMEM(tokens.shape, BF16),
            pltpu.VMEM((4, *w_query.shape), BF16),
            pltpu.SemaphoreType.DMA((5,)),
        ],
        compiler_params=PARAMS,
        interpret=INTERPRET,
        name="project",
    )(positions, *map(in_hbm, (tokens, w_query, w_key, w_value, w_gate)))
    near = lax.all_to_all(parts, "kv_1", 0, 0, tiled=True)
    near, turns = pl.pallas_call(
        first_sum_kernel,
        out_shape=[sds((NZ, proj, dim), BF16), sds((2, dim), F32)],
        in_specs=[smem, VMEM],
        out_specs=[VMEM, VMEM],
        scratch_shapes=[pltpu.VMEM((NZ, proj, dim), F32)],
        compiler_params=PARAMS,
        interpret=INTERPRET,
        name="near_sum",
    )(positions, near)
    far = along_z(near)
    updated, attended = kernel_call(
        retention_kernel,
        [sds(state.shape, F32), sds((SEQS, heads, dim), BF16)],
        3,
        name="retention",
    )(far, turns, state)
    gathered = lax.all_to_all(attended, ("kv_1", "kv_0"), 0, 0, tiled=True)
    gathered = lax.all_gather(gathered, "tp", axis=0)
    per = SEQS * cols // LANES
    mixed = kernel_call(
        mix_kernel,
        sds((NZ, per, LANES), BF16),
        3,
        scratch=[pltpu.VMEM((2, SEQS, heads, dim), F32)],
        name="mix",
    )(gathered.reshape(2, SEQS, heads, dim), w_out.T, tokens)
    rows = along_z(mixed)
    rows = jnp.broadcast_to(rows[None], (NY, *rows.shape))
    rows = lax.all_to_all(rows, "kv_1", 0, 0, tiled=True)
    rows = lax.all_gather(rows, "tp", axis=0)
    lines = half // LANES
    own, other, hidden_row, new_state = pl.pallas_call(
        feed_kernel,
        out_shape=[
            sds((SEQS, half), BF16),
            sds((SEQS, half), BF16),
            sds((1, width), F32),
            sds(state.shape, F32),
        ],
        in_specs=[VMEM] * 6,
        out_specs=[VMEM] * 3 + [pl.BlockSpec(memory_space=pl.ANY)],
        scratch_shapes=[
            pltpu.VMEM((SEQS, width), F32),
            pltpu.VMEM((SEQS, width), BF16),
            pltpu.VMEM((2, SEQS, LANES), F32),
            pltpu.SemaphoreType.DMA,
        ],
        compiler_params=PARAMS,
        interpret=INTERPRET,
        name="feed",
    )(rows, gain_mix[None, :], w_ffn_gate.T, w_ffn_up.T, w_ffn_down, updated)
    both = lax.all_gather(other, "tp", axis=0)
    part = kernel_call(pair_sum_kernel, sds(own.shape, BF16), 2, name="pair_sum")(own, both)
    part = lax.all_to_all(part.reshape(NY, NZ, half), "kv_1", 0, 0, tiled=True)
    part = kernel_call(
        near_sum_kernel,
        sds((NZ, lines, LANES), BF16),
        1,
        scratch=[pltpu.VMEM((NZ, lines, LANES), F32)],
        name="half_sum",
    )(part)
    part = along_z(part)
    summed = kernel_call(ffn_sum_kernel, sds((lines, LANES), F32), 2, name="ffn_sum")(
        part, hidden_row.reshape(2 * lines, LANES)
    )
    summed = lax.all_gather(summed, "tp", axis=0, tiled=True)
    spread = kernel_call(final_norm_kernel, sds((SEQS, LANES), F32), 2, name="final_norm")(
        summed, gain_out.reshape(2 * lines, LANES)
    )
    spread = lax.all_to_all(
        spread.reshape(SEQS, 1, LANES), KV_TP, 0, 0, tiled=True, axis_index_groups=ALL_GROUPS
    )
    layer_out = kernel_call(place_kernel, sds((cols, SEQS), BF16), 1, name="place")(
        spread.reshape(SEQS, LANES)
    )
    return (layer_out.T, new_state)


def solution(mesh):
    finer = Mesh(
        mesh.devices.reshape(mesh.shape["dp"], NZ, NY, mesh.shape["tp"]),
        ("dp", "kv_0", "kv_1", "tp"),
    )
    return jax.shard_map(
        on_device,
        mesh=finer,
        in_specs=(
            P("dp", KV),
            P(DP_KV),
            P(DP_KV, "tp", None, None),
            P(KV, "tp"),
            P(KV, "tp"),
            P(KV, "tp"),
            P(KV, "tp"),
            P(None, KV_TP),
            P(),
            P(None, KV_TP),
            P(None, KV_TP),
            P(KV_TP, None),
            P(),
        ),
        out_specs=(P("dp", KV_TP), P(DP_KV, "tp", None, None)),
        check_vma=False,
    )
```
